128 devices in a mesh: ep: 32 (over z, y, core), tp: 4 (over x).
Axes of the slice: x: 4, y: 4, z: 4, core: 2. Of those that a mesh axis runs over, the one named last changes fastest.
Arguments:
- queries: bfloat16 [32768, 1024], P('ep', 'tp'), may hold values from -6 to 6
- key_rows: bfloat16 [32768, 256], P('ep', 'tp'), may hold values from -6 to 6
- values: bfloat16 [32768, 256], P('ep', 'tp'), may hold values from -6 to 6
- sink_logit: float32 [16], P('tp'), may hold values from 3 to 7
- out_weight: bfloat16 [1024, 2048], P('tp'), may hold values from -0.1875 to 0.1875
- out_gain: float32 [2048], replicated, may hold values from 0.1 to 1.9
- routed_tokens: bfloat16 [65536, 2048], P(('ep', 'tp')), may hold values from -6 to 6
- expert_ids: int32 [65536, 2], P(('ep', 'tp')), may hold values from 0 to 31, as said below
- route_weight: float32 [65536, 2], P(('ep', 'tp')), may hold values from 0.1 to 1
- routed_gain: float32 [2048], replicated, may hold values from 0.1 to 1.9
- expert_gate: bfloat16 [32, 2048, 1024], P('ep', None, 'tp'), may hold values from -0.125 to 0.125
- expert_up: bfloat16 [32, 2048, 1024], P('ep', None, 'tp'), may hold values from -0.125 to 0.125
- expert_down: bfloat16 [32, 2048, 1024], P('ep', None, 'tp'), may hold values from -0.1875 to 0.1875
Outputs:
- mixer_out: bfloat16 [32768, 2048], P(('ep', 'tp'))
- experts_out: bfloat16 [65536, 2048], P(('ep', 'tp'))
The draws below stay inside these ranges and needn't reach their ends.
Inputs may be any that keep to these rules, and one draw needn't show every extreme that they name: `expert_ids`: both experts of a row lie in one group (equal id // 8); the 512 rows of one device name every group exactly 512 / 4 times; the rows of one device name no expert more than 64 times; in every device's rows some expert of each group is named exactly 64 times, and one expert is named exactly 64 times by the rows of every device.
All inputs are finite; a program needn't handle non-finite values.
Results may differ from the reference program's by a relative error of at most 0.0071.
Values may be sent and summed in bfloat16 or wider, within the bound.
A program may use at most 128 MiB of HBM per device.

```python
import math
import jax
import jax.numpy as jnp
from jax import lax

D = 2048
HEADS = 16
KV_HEADS = 4
HEAD_DIM = 64
WINDOW = 128
QBLOCK = 512
EXPERTS = 32
GROUPS = 4
EPG = 8
TOP = 2
EXPERT_FF = 1024
TB = 512
CAP = 64
SEQ_A = 32768
TOKENS_B = 65536
N_EP = 32
N_TP = 4


def draw_queries(key, part):
    drawn = jax.random.normal(jax.random.fold_in(key, 12), (SEQ_A, HEADS * HEAD_DIM), jnp.float32)
    return jnp.clip(drawn, -4.0, 4.0).astype(jnp.bfloat16)


def draw_key_rows(key, part):
    drawn = jax.random.normal(jax.random.fold_in(key, 22), (SEQ_A, KV_HEADS * HEAD_DIM), jnp.float32)
    return jnp.clip(drawn, -4.0, 4.0).astype(jnp.bfloat16)


def draw_expert_ids(key, part):
    block_total = TOKENS_B // TB
    half_group = TB // (2 * GROUPS)
    common_hot = jax.random.randint(jax.random.fold_in(key, 101), (), 0, EPG)

    def one_block(block_index):
        block_key = jax.random.fold_in(jax.random.fold_in(key, 202), block_index)
        order_key, hot_key, rest_key = jax.random.split(block_key, 3)
        order = jax.random.permutation(order_key, TB)
        hottest = jax.random.randint(hot_key, (GROUPS,), 0, EPG).at[0].set(common_hot)
        others = jax.vmap(lambda inner: jax.random.permutation(inner, EPG - 1))(jax.random.split(rest_key, GROUPS))
        group = order % GROUPS
        rank = order // GROUPS
        hot_token = hottest[group]
        rest_token = others[group]
        stride = 1 + rank // (EPG - 1) % (EPG - 2)
        first_other = jnp.take_along_axis(rest_token, (rank % (EPG - 1))[:, None], axis=1)[:, 0]
        second_other = jnp.take_along_axis(rest_token, ((rank + stride) % (EPG - 1))[:, None], axis=1)[:, 0]
        other_one = (hot_token + 1 + first_other) % EPG
        other_two = (hot_token + 1 + second_other) % EPG
        leading = jnp.where(rank < half_group, hot_token, other_one)
        trailing = jnp.where(rank < half_group, other_one, other_two)
        return jnp.stack([group * EPG + leading, group * EPG + trailing], axis=-1)
    chosen = jax.vmap(one_block)(jnp.arange(block_total))
    return chosen.reshape(TOKENS_B, TOP).astype(jnp.int32)


def block_scale(rng, dims, shards, least, high):
    gain = 1.0
    for dim, blocks in shards:
        steps = jax.random.uniform(jax.random.fold_in(jax.random.fold_in(rng, 6), dim), (blocks,), jnp.float32, least / len(shards), high / len(shards))
        gain = gain * jnp.repeat(jnp.exp(steps), dims[dim] // blocks).reshape((-1,) + (1,) * (len(dims) - 1 - dim))
    return gain


def gaussian(rng, shape, deviation, most, cuts=(), kind=jnp.bfloat16):
    level = block_scale(rng, shape, cuts, -0.22, 0.18) if cuts else 1.0
    values = jax.random.normal(rng, shape, jnp.float32) * deviation * level
    return jnp.minimum(jnp.maximum(values, -most), most).astype(kind)


def setup_inputs(seed: int = 0) -> dict:
    seeds = jax.random.split(jax.random.key(seed), 14)
    queries = draw_queries(jax.random.fold_in(seeds[13], 71), 0)
    key_rows = draw_key_rows(jax.random.fold_in(seeds[13], 71), 0)
    values = gaussian(seeds[2], (SEQ_A, KV_HEADS * HEAD_DIM), 1.0, 6.0, ((0, 32), (1, 4)))
    sink_logit = jnp.clip(3.0 + 4.0 * jax.random.uniform(seeds[3], (HEADS,), jnp.float32) ** block_scale(seeds[3], (HEADS,), ((0, 4),), -0.2, 0.2), 3.0, 7.0)
    out_weight = gaussian(seeds[4], (HEADS * HEAD_DIM, D), (HEADS * HEAD_DIM) ** -0.5, 0.1875, ((0, 4),))
    out_gain = jnp.clip(1.0 + 0.18 * jax.random.normal(seeds[5], (D,), jnp.float32), 0.1, 1.9)
    routed_tokens = gaussian(seeds[6], (TOKENS_B, D), 1.0, 6.0, ((0, 128),))
    expert_ids = draw_expert_ids(jax.random.fold_in(seeds[13], 71), 0)
    route_weight = jnp.clip(jnp.exp(math.log(1.0) - 2.3025851 * jax.random.uniform(seeds[8], (TOKENS_B, TOP), jnp.float32) ** block_scale(seeds[8], (TOKENS_B, TOP), ((0, 128),), -0.2, 0.2)), 0.1, 1.0)
    routed_gain = jnp.clip(1.0 + 0.18 * jax.random.normal(seeds[9], (D,), jnp.float32), 0.1, 1.9)
    expert_gate = gaussian(seeds[10], (EXPERTS, D, EXPERT_FF), D ** -0.5, 0.125, ((0, 32), (2, 4)))
    expert_up = gaussian(seeds[11], (EXPERTS, D, EXPERT_FF), D ** -0.5, 0.125, ((0, 32), (2, 4)))
    expert_down = gaussian(seeds[12], (EXPERTS, D, EXPERT_FF), EXPERT_FF ** -0.5, 0.1875, ((0, 32), (2, 4)))
    return dict(queries=queries, key_rows=key_rows, values=values, sink_logit=sink_logit, out_weight=out_weight, out_gain=out_gain, routed_tokens=routed_tokens, expert_ids=expert_ids, route_weight=route_weight, routed_gain=routed_gain, expert_gate=expert_gate, expert_up=expert_up, expert_down=expert_down)


epsilon = 1e-06
far_below = -1e+30

def window_block(block_index, grouped, padded_keys, padded_values, sink_logit, seq_total):
    start_row = block_index * QBLOCK
    span_keys = QBLOCK + 2 * WINDOW
    query_block = lax.dynamic_slice_in_dim(grouped, start_row, QBLOCK, 0).astype(jnp.float32)
    key_block = lax.dynamic_slice_in_dim(padded_keys, start_row, span_keys, 0).astype(jnp.float32)
    value_block = lax.dynamic_slice_in_dim(padded_values, start_row, span_keys, 0).astype(jnp.float32)
    scores = jnp.einsum('qhgd,khd->hgqk', query_block, key_block) * HEAD_DIM ** (-0.5)
    query_pos = start_row + jnp.arange(QBLOCK, dtype=jnp.int32)
    key_pos = start_row - WINDOW + jnp.arange(span_keys, dtype=jnp.int32)
    valid = (jnp.abs(key_pos[None, :] - query_pos[:, None]) <= WINDOW) & (key_pos[None, :] >= 0) & (key_pos[None, :] < seq_total)
    sinks = sink_logit.reshape(KV_HEADS, HEADS // KV_HEADS)[:, :, None, None]
    masked = jnp.where(valid, scores, far_below)
    largest = jnp.maximum(lax.optimization_barrier(jnp.max(masked, axis=-1, keepdims=True)), sinks)
    raised = jnp.where(valid, jnp.exp(masked - largest), 0.0)
    denominator = lax.optimization_barrier(jnp.sum(raised, axis=-1, keepdims=True)) + jnp.exp(sinks - largest)
    weights = (raised / denominator).astype(jnp.bfloat16)
    attended = jnp.einsum('hgqk,khd->qhgd', weights.astype(jnp.float32), value_block)
    return attended.astype(jnp.bfloat16).reshape(QBLOCK, HEADS * HEAD_DIM)

def reference(queries, key_rows, values, sink_logit, out_weight, out_gain, routed_tokens, expert_ids, route_weight, routed_gain, expert_gate, expert_up, expert_down):
    seq_total = queries.shape[0]
    grouped = queries.reshape(seq_total, KV_HEADS, HEADS // KV_HEADS, HEAD_DIM)
    padding = ((WINDOW, WINDOW), (0, 0), (0, 0))
    padded_keys = jnp.pad(key_rows.reshape(seq_total, KV_HEADS, HEAD_DIM), padding)
    padded_values = jnp.pad(values.reshape(seq_total, KV_HEADS, HEAD_DIM), padding)
    block_ids = jnp.arange(seq_total // QBLOCK, dtype=jnp.int32)
    attended = lax.map(lambda block_index: window_block(block_index, grouped, padded_keys, padded_values, sink_logit, seq_total), block_ids)
    attended = attended.reshape(seq_total, HEADS * HEAD_DIM)
    mixed = jnp.dot(attended, out_weight, preferred_element_type=jnp.float32)
    mixer_out = (mixed * lax.rsqrt(lax.optimization_barrier(jnp.mean(mixed * mixed, axis=-1, keepdims=True)) + epsilon) * out_gain).astype(jnp.bfloat16)
    token_total = routed_tokens.shape[0]
    inputs = routed_tokens.astype(jnp.float32)
    normed = (inputs * lax.rsqrt(lax.optimization_barrier(jnp.mean(inputs * inputs, axis=-1, keepdims=True)) + epsilon) * routed_gain).astype(jnp.bfloat16)
    flat_ids = expert_ids.reshape(-1)
    most_rows = CAP * N_EP * N_TP
    empty = jnp.zeros((token_total * TOP, normed.shape[1]), jnp.bfloat16)

    def one_expert(results, expert):
        picked = jnp.nonzero(flat_ids == expert, size=most_rows, fill_value=token_total * TOP)[0]
        rows_in = jnp.take(normed, picked // TOP, axis=0, mode='fill', fill_value=0)
        gate = jnp.dot(rows_in, expert_gate[expert], preferred_element_type=jnp.float32)
        upward = jnp.dot(rows_in, expert_up[expert], preferred_element_type=jnp.float32)
        hidden = (jax.nn.silu(gate) * upward).astype(jnp.bfloat16)
        produced = jnp.dot(hidden, expert_down[expert].T, preferred_element_type=jnp.float32).astype(jnp.bfloat16)
        return (results.at[picked].set(produced, mode='drop'), None)
    results, unused = lax.scan(one_expert, empty, jnp.arange(EXPERTS, dtype=jnp.int32))
    results = results.reshape(token_total, TOP, normed.shape[1]).astype(jnp.float32)
    experts_out = lax.optimization_barrier(jnp.sum(results * route_weight[:, :, None], axis=1)).astype(jnp.bfloat16)
    return (mixer_out, experts_out)
```

```python
import jax
import jax.numpy as jnp
from jax import lax
from jax.experimental import pallas as pl
from jax.experimental.pallas import tpu as pltpu
from jax.sharding import PartitionSpec as P

F32, BF16 = jnp.float32, jnp.bfloat16
MESH = pl.DeviceIdType.MESH
D = 2048
WINDOW = 128
SEQ = 32768
EPS = 1e-06
COPIES = 128


def dot(a, b):
    return lax.dot_general(a, b, (((1,), (0,)), ((), ())), preferred_element_type=F32)


def dot_nt(a, b):
    return lax.dot_general(a, b, (((1,), (1,)), ((), ())), preferred_element_type=F32)


def iota(shape, dim):
    return lax.broadcasted_iota(jnp.int32, shape, dim)


def kernel(
    q_in, kv_in, sink, ow_in, og, tok_in, meta, rg, wg_in, wu_in, wd_in,
    mix_out, exp_out,
    W, OW, T, X, H, R, FB, S, OUT, WS, PT, PM, MT, MS, Q, KV, ATT, AR, MX,
    ready, lsem, ssem, rsem,
):
    ep = lax.axis_index("ep")
    tp = lax.axis_index("tp")
    core, y, z = ep % 2, (ep // 2) % 4, ep // 8

    def place(z, y, core):
        return (z * 4 + y) * 2 + core

    xr, xl, xo = (ep, (tp + 1) % 4), (ep, (tp + 3) % 4), (ep, (tp + 2) % 4)
    yr, yl = (place(z, (y + 1) % 4, core), tp), (place(z, (y + 3) % 4, core), tp)
    zr, zl, zo = (
        (place((z + 1) % 4, y, core), tp),
        (place((z + 3) % 4, y, core), tp),
        (place((z + 2) % 4, y, core), tp),
    )
    sib = (place(z, y, 1 - core), tp)
    after, before = ((ep + 1) % 32, tp), ((ep + 31) % 32, tp)

    numbers = {}
    unsent = {}

    def send(name, src, dst, dev):
        n = numbers.setdefault(name, len(numbers))
        copy = pltpu.make_async_remote_copy(
            src_ref=src, dst_ref=dst, send_sem=ssem.at[n], recv_sem=rsem.at[n],
            device_id=dev, device_id_type=MESH,
        )
        copy.start()
        unsent[name] = copy
        copies[name] = copy

    copies = {}

    def got(name):
        copies[name].wait_recv()

    def sent(prefix):
        for name in [n for n in unsent if n.startswith(prefix)]:
            unsent.pop(name).wait_send()

    here = [
        pltpu.make_async_copy(src, dst, lsem.at[i])
        for i, (src, dst) in enumerate([
            (wg_in, W.at[0, 0]),
            (wu_in, W.at[1, 0]),
            (wd_in, W.at[2, 0]),
            (tok_in, X.at[3]),
            (kv_in, KV.at[WINDOW : WINDOW + 1024]),
            (q_in, Q),
            (ow_in, OW.at[0]),
        ])
    ]
    for copy in here:
        copy.start()
    barrier = pltpu.get_barrier_semaphore()
    near = (xr, xl, xo, yr, yl, zr, zl, zo, sib, after, before)
    for dev in near:
        pl.semaphore_signal(barrier, inc=1, device_id=dev, device_id_type=MESH)
    pl.semaphore_wait(barrier, len(near))

    for m in range(3):
        here[m].wait()
        send(f"x{m}r", W.at[m, 0], W.at[m, 1], xr)
        send(f"x{m}l", W.at[m, 0], W.at[m, 2], xl)

    def pass_weight(m):
        got(f"x{m}r")
        send(f"x{m}fr", W.at[m, 1, 0:1024], W.at[m, 3, 0:1024], xr)
        got(f"x{m}l")
        send(f"x{m}fl", W.at[m, 2, 1024:2048], W.at[m, 3, 1024:2048], xl)

    here[4].wait()
    send("halo_n", KV.at[1024 : 1024 + WINDOW], KV.at[0:WINDOW], after)
    send("halo_p", KV.at[WINDOW : 2 * WINDOW], KV.at[1024 + WINDOW :], before)

    id0, id1 = meta[0:1, :], meta[1:2, :]
    w0, w1 = meta[2:3, :], meta[3:4, :]
    ie = iota((32, 512), 0).astype(F32)
    one0 = jnp.where(ie == id0, 1.0, 0.0)
    one1 = jnp.where(ie == id1, 1.0, 0.0)
    upper = jnp.where(iota((512, 512), 0) < iota((512, 512), 1), 1.0, 0.0).astype(BF16)
    ahead = dot((one0 + one1).astype(BF16), upper)
    slot0 = jnp.sum(ahead * one0, axis=0, keepdims=True)
    slot1 = jnp.sum(ahead * one1, axis=0, keepdims=True) + jnp.where(id0 == id1, 1.0, 0.0)
    gid = jnp.floor(id0 * 0.125)
    oneg = jnp.where(iota((8, 512), 0).astype(F32) == gid, 1.0, 0.0)
    rank = jnp.sum(dot(oneg.astype(BF16), upper) * oneg, axis=0, keepdims=True)
    dest = gid * 128.0 + rank

    def split(w):
        high = w.astype(BF16).astype(F32)
        mid = (w - high).astype(BF16).astype(F32)
        return high, mid, w - high - mid

    rows16 = iota((16, 512), 0)
    m16 = jnp.zeros((16, 512), F32)
    for i, row in enumerate((id0, slot0, id1, slot1, *split(w0), *split(w1))):
        m16 = jnp.where(rows16 == i, row, m16)
    m16 = m16.astype(BF16)
    for kp in range(4):
        base = ((z + kp) % 4) * 128
        pm = jnp.where((iota((128, 512), 0) + base).astype(F32) == dest, 1.0, 0.0)
        PM[kp] = pm.astype(BF16)
        moved = dot_nt(m16, pm.astype(BF16))
        if kp == 0:
            MT[0, 0, 0] = moved
        else:
            MS[kp - 1] = moved
    for kp, dev in ((1, zr), (3, zl), (2, zo)):
        send(f"mz{kp}", MS.at[kp - 1], MT.at[0, 0, (4 - kp) % 4], dev)

    here[3].wait()

    @pl.loop(0, 16)
    def _(i):
        r = pl.ds(pl.multiple_of(i * 32, 32), 32)
        v = X[3, r, :].astype(F32)
        scale = lax.rsqrt(jnp.mean(v * v, axis=-1, keepdims=True) + EPS)
        X[2, r, :] = (v * scale * rg[...]).astype(BF16)

    for kp in (0, 1, 3, 2):
        @pl.loop(0, 4)
        def _(n):
            c = pl.ds(pl.multiple_of(n * 512, 512), 512)
            tile = dot(PM[kp], X[2, :, c]).astype(BF16)
            if kp == 0:
                T[0, 0, 0:128, c] = tile
            else:
                S[kp - 1, :, c] = tile

        if kp:
            dev = {1: zr, 2: zo, 3: zl}[kp]
            send(f"z{kp}", S.at[kp - 1], T.at[(4 - kp) % 4, 0, 0:128], dev)
        else:
            send("y0r", T.at[0, 0, 0:128], T.at[0, 3, 0:128], yr)
            send("y0l", T.at[0, 0, 0:128], T.at[0, 1, 0:128], yl)
            send("d00", T.at[0, 0, 0:128], T.at[0, 0, 128:256], sib)

    def gather_start(k):
        got(f"z{(4 - k) % 4}")
        send(f"y{k}r", T.at[k, 0, 0:128], T.at[k, 3, 0:128], yr)
        send(f"y{k}l", T.at[k, 0, 0:128], T.at[k, 1, 0:128], yl)
        send(f"d{k}0", T.at[k, 0, 0:128], T.at[k, 0, 128:256], sib)

    def gather_pass(k):
        got(f"y{k}r")
        send(f"y{k}fr", T.at[k, 3, 0:64], T.at[k, 2, 0:64], yr)
        send(f"d{k}3", T.at[k, 3, 0:128], T.at[k, 3, 128:256], sib)
        got(f"y{k}l")
        send(f"y{k}fl", T.at[k, 1, 64:128], T.at[k, 2, 64:128], yl)
        send(f"d{k}1", T.at[k, 1, 0:128], T.at[k, 1, 128:256], sib)

    def gather_end(k):
        got(f"y{k}fr")
        got(f"y{k}fl")
        send(f"d{k}2", T.at[k, 2, 0:128], T.at[k, 2, 128:256], sib)

    for kp in (1, 3, 2):
        got(f"mz{kp}")
    send("myr", MT.at[0, 0], MT.at[0, 3], yr)
    send("myl", MT.at[0, 0], MT.at[0, 1], yl)

    here[5].wait()
    got("halo_n")
    got("halo_p")
    lane = iota((128, 128), 1)
    r_pos = iota((128, 384), 0)
    c_pos = iota((128, 384), 1)
    gap = c_pos - r_pos

    @pl.loop(0, 8)
    def _(b):
        r0 = pl.multiple_of(b * 128, 128)
        kk = KV[pl.ds(r0, 384), 0:128]
        vv = KV[pl.ds(r0, 384), 128:256]
        key = c_pos + (ep * 1024 + b * 128 - WINDOW)
        valid = (gap >= 0) & (gap <= 2 * WINDOW) & (key >= 0) & (key < SEQ)
        found = []
        for h in range(4):
            qh = Q[pl.ds(r0, 128), (h // 2) * 128 : (h // 2) * 128 + 128]
            qh = jnp.where((lane < 64) if h % 2 == 0 else (lane >= 64), qh, 0.0).astype(BF16)
            s = dot_nt(qh, kk) * 0.125
            s = jnp.where(valid, s, -1e30)
            largest = jnp.maximum(jnp.max(s, axis=-1, keepdims=True), sink[h])
            e = jnp.where(valid, jnp.exp(s - largest), 0.0)
            total = jnp.sum(e, axis=-1, keepdims=True) + jnp.exp(sink[h] - largest)
            found.append(dot((e / total).astype(BF16), vv))
        ATT[pl.ds(r0, 128), 0:128] = jnp.where(lane < 64, found[0], found[1]).astype(BF16)
        ATT[pl.ds(r0, 128), 128:256] = jnp.where(lane < 64, found[2], found[3]).astype(BF16)

    got("myr")
    send("myf", MT.at[0, 3], MT.at[0, 2], yr)
    got("myl")

    me = ep.astype(F32)

    def pack(k):
        @pl.loop(0, 4)
        def _(j):
            m0, m1 = MT[0, j, k], MT[1, j, k]
            both = jnp.concatenate([m0, m1], axis=1)
            shift = jnp.where(iota((1, 256), 1) >= 128, 64.0, 0.0)
            sl0 = jnp.where(both[0:1] == me, both[1:2] + shift, -1.0)
            sl1 = jnp.where(both[2:3] == me, both[3:4] + shift, -1.0)
            wt0 = both[4:5] + both[5:6] + both[6:7]
            wt1 = both[7:8] + both[8:9] + both[9:10]
            rows = iota((128, 256), 0).astype(F32)
            is0, is1 = rows == sl0, rows == sl1
            pick = jnp.where(is0 | is1, 1.0, 0.0)
            weight = jnp.sum(jnp.where(is0, wt0, 0.0) + jnp.where(is1, wt1, 0.0), axis=1, keepdims=True)
            r = pl.ds(pl.multiple_of(j * 128, 128), 128)
            WS[k, r, :] = jnp.broadcast_to(weight, (128, 128))
            PT[k, j] = jnp.transpose(pick).astype(BF16)
            pick = pick.astype(BF16)
            for n in range(4):
                X[k, r, n * 512 : n * 512 + 512] = dot(
                    pick, T[k, j, :, n * 512 : n * 512 + 512]
                ).astype(BF16)

    def gate_up(first, last):
        @pl.loop(first * 4, last * 4)
        def _(i):
            s, k = i // 4, i % 4
            g = dot(X[k], W[0, s])
            u = dot(X[k], W[1, s])
            H[k, s] = (g / (1.0 + jnp.exp(-g)) * u).astype(BF16)

    gather_pass(0)
    gather_start(1)
    gather_start(3)
    pass_weight(0)
    gather_end(0)
    got("myf")
    send("md", MT.at[0], MT.at[1], sib)
    got("md")
    for j in (0, 3, 1, 2):
        got(f"d0{j}")
    pack(0)
    gather_start(2)
    gather_pass(1)
    gather_end(1)
    pass_weight(1)
    for j in (0, 3, 1, 2):
        got(f"d1{j}")
    pack(1)
    gather_pass(3)
    gather_end(3)
    for j in (0, 3, 1, 2):
        got(f"d3{j}")
    pack(3)
    gather_pass(2)
    pass_weight(2)
    here[6].wait()
    send("owr", OW.at[0], OW.at[1], xr)
    send("owl", OW.at[0], OW.at[2], xl)
    for name, d, slot, dev in (("ar", 1, 1, xr), ("al", 3, 2, xl), ("ao", 2, 3, xo)):
        part = pl.ds(pl.multiple_of(((tp + d) % 4) * 256, 256), 256)
        send(name, ATT.at[part], AR.at[slot], dev)
    gather_end(2)
    for j in (0, 3, 1, 2):
        got(f"d2{j}")
    pack(2)
    sent("y")
    sent("d")
    pl.semaphore_signal(ready, inc=1, device_id=sib, device_id_type=MESH)
    gate_up(0, 3)
    for m in (0, 1):
        got(f"x{m}fr")
        got(f"x{m}fl")
    gate_up(3, 4)
    got("x2fr")
    got("x2fl")
    pl.semaphore_wait(ready, 1)

    def down(k):
        @pl.loop(0, 8)
        def _(n):
            c = pl.ds(pl.multiple_of(n * 256, 256), 256)
            out = dot_nt(H[k, 0], W[2, 0, c, :])
            for s in range(1, 4):
                out += dot_nt(H[k, s], W[2, s, c, :])
            scale = WS[k]
            scale = jnp.concatenate([scale, scale], axis=1)
            scaled = (out.astype(BF16).astype(F32) * scale).astype(BF16)
            for j in range(4):
                part = dot(PT[k, j], scaled[j * 128 : j * 128 + 128])
                X[k, j * 128 : j * 128 + 128, c] = part[0:128].astype(BF16)
                T[k, j, 128:256, c] = part[128:256].astype(BF16)

        send(f"r{k}", T.at[k, :, 128:256], T.at[k, :, 0:128], sib)

    def plus(count, out, *terms):
        @pl.loop(0, count // 16)
        def _(i):
            r = pl.multiple_of(i * 16, 16)
            total = None
            for ref, lead, base in terms:
                term = ref[(*lead, pl.ds(base + r, 16), slice(None))].astype(F32)
                total = term if total is None else total + term
            ref, lead, base = out
            ref[(*lead, pl.ds(base + r, 16), slice(None))] = total.astype(BF16)

    def early(k):
        got(f"r{k}")
        for j in (2, 1, 3, 0):
            plus(128, (X, (k,), j * 128), (X, (k,), j * 128), (T, (k, j), 0))
            if j == 2:
                send(f"b{k}hr", X.at[k, 256:320], R.at[k, 0], yr)
                send(f"b{k}hl", X.at[k, 320:384], R.at[k, 1], yl)
            if j == 1:
                send(f"b{k}er", X.at[k, 192:256], FB.at[k, 0, 64:128], yr)
            if j == 3:
                send(f"b{k}el", X.at[k, 384:448], FB.at[k, 1, 0:64], yl)

    def late(k):
        got(f"b{k}hr")
        plus(64, (X, (k,), 128), (X, (k,), 128), (R, (k, 0), 0))
        send(f"b{k}fr", X.at[k, 128:192], FB.at[k, 0, 0:64], yr)
        got(f"b{k}hl")
        plus(64, (X, (k,), 448), (X, (k,), 448), (R, (k, 1), 0))
        send(f"b{k}fl", X.at[k, 448:512], FB.at[k, 1, 64:128], yl)

    def finish(k):
        for half in ("er", "el", "fr", "fl"):
            got(f"b{k}{half}")
        out = (OUT, (0,), 0) if k == 0 else (S, (k - 1,), 0)
        plus(128, out, (X, (k,), 0), (FB, (k, 0), 0), (FB, (k, 1), 0))
        if k:
            send(f"f{k}", S.at[k - 1], OUT.at[(4 - k) % 4], {1: zr, 2: zo, 3: zl}[k])

    sent("z")
    down(2)
    early(2)
    down(1)
    late(2)
    early(1)
    down(3)
    finish(2)
    late(1)
    early(3)
    down(0)
    got("owr")
    send("owfr", OW.at[1, 0:128], OW.at[3, 0:128], xr)
    got("owl")
    send("owfl", OW.at[2, 128:256], OW.at[3, 128:256], xl)
    finish(1)
    late(3)
    early(0)
    late(0)

    for name in ("ar", "al", "ao", "owfr", "owfl"):
        got(name)
    own = pl.multiple_of(tp * 256, 256)
    AR[0] = ATT[pl.ds(own, 256), :]

    @pl.loop(0, 4)
    def _(i):
        r = pl.ds(pl.multiple_of(i * 64, 64), 64)
        mixed = dot(AR[0, r, :], OW[0])
        for s in range(1, 4):
            mixed += dot(AR[s, r, :], OW[s])
        scale = lax.rsqrt(jnp.mean(mixed * mixed, axis=-1, keepdims=True) + EPS)
        MX[r, :] = (mixed * scale * og[...]).astype(BF16)

    back = pltpu.make_async_copy(MX, mix_out, lsem.at[7])
    back.start()
    finish(3)
    for kp in range(4):
        PT[kp // 2, 2 * (kp % 2)] = jnp.transpose(PM[kp, :, 0:256].astype(F32)).astype(BF16)
        PT[kp // 2, 2 * (kp % 2) + 1] = jnp.transpose(PM[kp, :, 256:512].astype(F32)).astype(BF16)
    finish(0)
    for k in (2, 1, 3):
        got(f"f{k}")
    sent("b1")

    @pl.loop(0, 4)
    def _(n):
        c = pl.ds(pl.multiple_of(n * 512, 512), 512)
        for half in range(2):
            total = None
            for kp in range(4):
                part = dot(PT[kp // 2, 2 * (kp % 2) + half], OUT[kp, :, c])
                total = part if total is None else total + part
            X[1, half * 256 : half * 256 + 256, c] = total.astype(BF16)

    home = pltpu.make_async_copy(X.at[1], exp_out, lsem.at[8])
    home.start()
    sent("")
    home.wait()
    back.wait()


def local(
    queries, key_rows, values, sink_logit, out_weight, out_gain, routed_tokens,
    expert_ids, route_weight, routed_gain, expert_gate, expert_up, expert_down,
):
    kv = jnp.concatenate((key_rows, key_rows, values, values), axis=1)
    meta = jnp.concatenate((expert_ids.astype(F32), route_weight), axis=1).T
    anywhere = pl.BlockSpec(memory_space=pl.ANY)
    vmem = pl.BlockSpec(memory_space=pltpu.VMEM)
    smem = pl.BlockSpec(memory_space=pltpu.SMEM)
    scratch = [
        pltpu.VMEM((3, 4, 2048, 256), BF16),
        pltpu.VMEM((4, 256, D), BF16),
        pltpu.VMEM((4, 4, 256, D), BF16),
        pltpu.VMEM((4, 512, D), BF16),
        pltpu.VMEM((4, 4, 512, 256), BF16),
        pltpu.VMEM((4, 2, 64, D), BF16),
        pltpu.VMEM((4, 2, 128, D), BF16),
        pltpu.VMEM((3, 128, D), BF16),
        pltpu.VMEM((4, 128, D), BF16),
        pltpu.VMEM((4, 512, 128), F32),
        pltpu.VMEM((4, 4, 256, 128), BF16),
        pltpu.VMEM((4, 128, 512), BF16),
        pltpu.VMEM((2, 4, 4, 16, 128), F32),
        pltpu.VMEM((3, 16, 128), F32),
        pltpu.VMEM((1024, 256), BF16),
        pltpu.VMEM((1024 + 2 * WINDOW, 256), BF16),
        pltpu.VMEM((1024, 256), BF16),
        pltpu.VMEM((4, 256, 256), BF16),
        pltpu.VMEM((256, D), BF16),
        pltpu.SemaphoreType.REGULAR,
        pltpu.SemaphoreType.DMA((9,)),
        pltpu.SemaphoreType.DMA((COPIES,)),
        pltpu.SemaphoreType.DMA((COPIES,)),
    ]
    return pl.pallas_call(
        kernel,
        out_shape=(
            jax.ShapeDtypeStruct((256, D), BF16),
            jax.ShapeDtypeStruct((512, D), BF16),
        ),
        in_specs=[anywhere, anywhere, smem, anywhere, vmem, anywhere, vmem, vmem, anywhere, anywhere, anywhere],
        out_specs=(anywhere, anywhere),
        scratch_shapes=scratch,
        compiler_params=pltpu.CompilerParams(
            collective_id=0, has_side_effects=True, vmem_limit_bytes=67043328
        ),
        name="block",
    )(
        queries, kv, sink_logit, out_weight, out_gain.reshape(1, D), routed_tokens, meta,
        routed_gain.reshape(1, D), expert_gate.reshape(D, 256), expert_up.reshape(D, 256),
        expert_down.reshape(D, 256),
    )


def solution(mesh):
    placed = (
        P("ep", "tp"), P("ep", "tp"), P("ep", "tp"), P("tp"), P("tp", None), P(),
        P(("ep", "tp"), None), P(("ep", "tp"), None), P(("ep", "tp"), None), P(),
        P("ep", None, "tp"), P("ep", None, "tp"), P("ep", None, "tp"),
    )
    return jax.shard_map(
        local,
        mesh=mesh,
        in_specs=placed,
        out_specs=(P(("ep", "tp"), None), P(("ep", "tp"), None)),
        check_vma=False,
    )
```

```python
import jax
import jax.numpy as jnp
from jax import lax
from jax.experimental import pallas as pl
from jax.experimental.pallas import tpu as pltpu
from jax.sharding import PartitionSpec as P

F32, BF16 = jnp.float32, jnp.bfloat16
MESH = pl.DeviceIdType.MESH
D = 2048
WINDOW = 128
SEQ = 32768
EPS = 1e-06
COPIES = 117
SENDS = 56


def dot(a, b):
    return lax.dot_general(a, b, (((1,), (0,)), ((), ())), preferred_element_type=F32)


def dot_nt(a, b):
    return lax.dot_general(a, b, (((1,), (1,)), ((), ())), preferred_element_type=F32)


def iota(shape, dim):
    return lax.broadcasted_iota(jnp.int32, shape, dim)


CHUNKS = ((0, 256), (256, 256), (512, 512), (1024, 512), (1536, 512))


def kernel(
    q_in, k_in, v_in, sink, ow_in, og_in, tok_in, ids, rw, rg_in, wg_in, wu_in, wd_in,
    mix_out, exp_out,
    W, OW, T, X, H, R, FB, S, OUT, WS, PT, PM, PMT, MT, MS, Q, KV, ATT, AR, OG, RG,
    ready, lsem, ssem, rsem,
):
    ep = lax.axis_index("ep")
    tp = lax.axis_index("tp")
    core, y, z = ep % 2, (ep // 2) % 4, ep // 8

    def place(z, y, core):
        return (z * 4 + y) * 2 + core

    xr, xl, xo = (ep, (tp + 1) % 4), (ep, (tp + 3) % 4), (ep, (tp + 2) % 4)
    yr, yl = (place(z, (y + 1) % 4, core), tp), (place(z, (y + 3) % 4, core), tp)
    yo = (place(z, (y + 2) % 4, core), tp)
    zs = {d: (place((z + d) % 4, y, core), tp) for d in (1, 2, 3)}
    sib = (place(z, y, 1 - core), tp)
    after, before = ((ep + 1) % 32, tp), ((ep + 31) % 32, tp)

    numbers, unsent, copies, groups = {}, {}, {}, {}
    free = list(range(SENDS))[::-1]

    def send(name, src, dst, dev, into=None, group=None):
        if group in groups:
            n = groups[group]
        else:
            n = free.pop()
        copy = pltpu.make_async_remote_copy(
            src_ref=src, dst_ref=dst, send_sem=ssem.at[n],
            recv_sem=rsem.at[numbers.setdefault(into or name, len(numbers))],
            device_id=dev, device_id_type=MESH,
        )
        copy.start()
        assert name not in copies
        copies[name] = copy
        if group:
            groups[group] = n
        else:
            unsent[name] = copy, n

    def got(*names):
        for name in names:
            with jax.named_scope("got_" + name):
                copies[name].wait_recv()

    def whole(ref, n, m):
        return pltpu.make_async_remote_copy(
            src_ref=ref, dst_ref=ref, send_sem=ssem.at[n], recv_sem=rsem.at[m],
            device_id=sib, device_id_type=MESH,
        )

    def got_all(into, ref):
        with jax.named_scope("got_" + into):
            whole(ref, 0, numbers[into]).wait_recv()

    def sent(prefix):
        with jax.named_scope("sent_" + prefix):
            for name in [n for n in unsent if n.startswith(prefix)]:
                copy, n = unsent.pop(name)
                copy.wait_send()
                free.append(n)

    def sent_all(group, ref):
        with jax.named_scope("sent_" + group):
            n = groups.pop(group)
            whole(ref, n, 0).wait_send()
            free.append(n)

    def local(i, src, dst):
        copy = pltpu.make_async_copy(src, dst, lsem.at[i])
        copy.start()
        return copy

    here = [
        local(i, src, dst)
        for i, (src, dst) in enumerate([
            (wg_in, W.at[0, 0]),
            (tok_in, X.at[3]),
            (rg_in, RG),
            (wu_in, W.at[1, 0]),
            (q_in, Q),
            (wd_in, W.at[2, 0]),
            (ow_in, OW.at[0]),
            (og_in, OG),
        ])
    ]
    ours = slice(WINDOW, WINDOW + 1024)
    rows_here = [
        local(8 + 2 * i + half, src, KV.at[i, half * 64 : half * 64 + 64, ours])
        for i, src in enumerate((k_in, v_in))
        for half in range(2)
    ]
    near = (xr, xl, xo, yr, yl, yo, zs[1], zs[2], zs[3], sib, after, before)
    barrier = pltpu.get_barrier_semaphore()
    for dev in near:
        pl.semaphore_signal(barrier, inc=1, device_id=dev, device_id_type=MESH)

    def pass_weight(m):
        got(f"x{m}r")
        send(f"x{m}fr", W.at[m, 1, 0:1024], W.at[m, 3, 0:1024], xr, f"x{m}f")
        got(f"x{m}l")
        send(f"x{m}fl", W.at[m, 2, 1024:2048], W.at[m, 3, 1024:2048], xl, f"x{m}f")

    def start_down(c):
        rows = slice(CHUNKS[c][0], sum(CHUNKS[c]))
        send(f"w{c}r", W.at[2, 0, rows], W.at[2, 1, rows], xr)
        send(f"w{c}l", W.at[2, 0, rows], W.at[2, 2, rows], xl)

    def pass_down(c):
        first, width = CHUNKS[c]
        low, high = slice(first, first + width // 2), slice(first + width // 2, first + width)
        got(f"w{c}r")
        send(f"w{c}fr", W.at[2, 1, low], W.at[2, 3, low], xr, f"w{c}f")
        got(f"w{c}l")
        send(f"w{c}fl", W.at[2, 2, high], W.at[2, 3, high], xl, f"w{c}f")

    with jax.named_scope("routing"):
        id0, id1 = ids[0:1, :].astype(F32), ids[1:2, :].astype(F32)
        w0, w1 = rw[0:1, :], rw[1:2, :]
        ie = iota((32, 512), 0).astype(F32)
        one0 = jnp.where(ie == id0, 1.0, 0.0)
        one1 = jnp.where(ie == id1, 1.0, 0.0)
        upper = jnp.where(iota((512, 512), 0) < iota((512, 512), 1), 1.0, 0.0).astype(BF16)
        ahead = dot((one0 + one1).astype(BF16), upper)
        slot0 = jnp.sum(ahead * one0, axis=0, keepdims=True)
        slot1 = jnp.sum(ahead * one1, axis=0, keepdims=True) + jnp.where(id0 == id1, 1.0, 0.0)
        gid = jnp.floor(id0 * 0.125)
        oneg = jnp.where(iota((8, 512), 0).astype(F32) == gid, 1.0, 0.0)
        rank = jnp.sum(dot(oneg.astype(BF16), upper) * oneg, axis=0, keepdims=True)
        dest = gid * 128.0 + rank

        def split(w):
            high = w.astype(BF16).astype(F32)
            mid = (w - high).astype(BF16).astype(F32)
            return high, mid, w - high - mid

        rows16 = iota((16, 512), 0)
        m16 = jnp.zeros((16, 512), F32)
        for i, row in enumerate((id0, slot0, id1, slot1, *split(w0), *split(w1))):
            m16 = jnp.where(rows16 == i, row, m16)
        m16 = m16.astype(BF16)
        for kp in range(4):
            base = ((z + kp) % 4) * 128
            pm = jnp.where((iota((128, 512), 0) + base).astype(F32) == dest, 1.0, 0.0)
            PM[kp] = pm.astype(BF16)
            moved = dot_nt(m16, pm.astype(BF16))
            if kp == 0:
                MT[0, 0, 0] = moved
            else:
                MS[kp - 1] = moved
    with jax.named_scope("barrier"):
        pl.semaphore_wait(barrier, len(near))

    def start_weight(m, copy):
        copy.wait()
        send(f"x{m}r", W.at[m, 0], W.at[m, 1], xr)
        send(f"x{m}l", W.at[m, 0], W.at[m, 2], xl)

    start_weight(0, here[0])
    here[1].wait()
    here[2].wait()
    def shared(k):
        return None if k == 2 else f"d{k}"

    def start_tile(k):
        send(f"y{k}r", T.at[k, 0, 0:128], T.at[k, 3, 0:128], yr)
        send(f"y{k}l", T.at[k, 0, 0:128], T.at[k, 1, 0:128], yl)
        send(f"d{k}0", T.at[k, 0, 0:128], T.at[k, 0, 128:256], sib, shared(k))

    def permute(kp):
        with jax.named_scope(f"permute_{kp}"):
            v = dot(PM[kp], X[3])
            scale = lax.rsqrt(jnp.mean(v * v, axis=-1, keepdims=True) + EPS)
            tile = (v * scale * RG[...]).astype(BF16)
            if kp == 0:
                T[0, 0, 0:128] = tile
            else:
                S[kp - 1] = tile

    def send_tile(kp):
        send(f"z{kp}", S.at[kp - 1], T.at[4 - kp, 0, 0:128], zs[kp])

    permute(0)
    for kp in (1, 3, 2):
        send(f"mz{kp}", MS.at[kp - 1], MT.at[0, 0, 4 - kp], zs[kp], "mz")
    for copy in rows_here:
        copy.wait()
    send("halo_n", KV.at[:, :, 1024 : 1024 + WINDOW], KV.at[:, :, 0:WINDOW], after, "halo")
    send("halo_p", KV.at[:, :, WINDOW : 2 * WINDOW], KV.at[:, :, 1024 + WINDOW :], before, "halo")
    start_tile(0)
    start_weight(1, here[3])
    here[5].wait()
    start_down(0)
    for kp in (1, 3):
        permute(kp)
        send_tile(kp)
    permute(2)

    def gather_start(k):
        got(f"z{4 - k}")
        start_tile(k)

    def gather_pass(k):
        got(f"y{k}r")
        send(f"y{k}fr", T.at[k, 3, 0:64], T.at[k, 2, 0:64], yr, f"y{k}f")
        send(f"d{k}3", T.at[k, 3, 0:128], T.at[k, 3, 128:256], sib, shared(k))
        got(f"y{k}l")
        send(f"y{k}fl", T.at[k, 1, 64:128], T.at[k, 2, 64:128], yl, f"y{k}f")
        send(f"d{k}1", T.at[k, 1, 0:128], T.at[k, 1, 128:256], sib, shared(k))

    def gather_end(k):
        got_all(f"y{k}f", T.at[k, 2, 0:128])
        send(f"d{k}2", T.at[k, 2, 0:128], T.at[k, 2, 128:256], sib, shared(k))

    def attend(first, last):
        lane = iota((128, 128), 1)
        c_pos = iota((128, 384), 1)
        gap = c_pos - iota((128, 384), 0)

        @pl.loop(first, last)
        def _(i):
            b = (i + 1) % 8
            r0 = pl.multiple_of(b * 128, 128)
            kk = KV[0, :, pl.ds(r0, 384)]
            vv = KV[1, :, pl.ds(r0, 384)]
            key = c_pos + (ep * 1024 + b * 128 - WINDOW)
            valid = (gap >= 0) & (gap <= 2 * WINDOW) & (key >= 0) & (key < SEQ)
            found = []
            for h in range(4):
                qh = Q[pl.ds(r0, 128), (h // 2) * 128 : (h // 2) * 128 + 128]
                qh = jnp.where((lane < 64) if h % 2 == 0 else (lane >= 64), qh, 0.0).astype(BF16)
                s = dot(qh, kk) * 0.125
                s = jnp.where(valid, s, -1e30)
                largest = jnp.maximum(jnp.max(s, axis=-1, keepdims=True), sink[h])
                e = jnp.where(valid, jnp.exp(s - largest), 0.0)
                total = jnp.sum(e, axis=-1, keepdims=True) + jnp.exp(sink[h] - largest)
                found.append(dot_nt((e / total).astype(BF16), vv))
            ATT[pl.ds(r0, 128), 0:128] = jnp.where(lane < 64, found[0], found[1]).astype(BF16)
            ATT[pl.ds(r0, 128), 128:256] = jnp.where(lane < 64, found[2], found[3]).astype(BF16)

    me = ep.astype(F32)

    def pack(k, first=0, last=4):
        with jax.named_scope(f"pack_{k}"):
            @pl.loop(first, last)
            def _(j):
                both = jnp.concatenate([MT[0, j, k], MT[1, j, k]], axis=1)
                shift = jnp.where(iota((1, 256), 1) >= 128, 64.0, 0.0)
                sl0 = jnp.where(both[0:1] == me, both[1:2] + shift, -1.0)
                sl1 = jnp.where(both[2:3] == me, both[3:4] + shift, -1.0)
                wt0 = both[4:5] + both[5:6] + both[6:7]
                wt1 = both[7:8] + both[8:9] + both[9:10]
                rows = iota((128, 256), 0).astype(F32)
                is0, is1 = rows == sl0, rows == sl1
                pick = jnp.where(is0 | is1, 1.0, 0.0)
                weight = jnp.sum(jnp.where(is0, wt0, 0.0) + jnp.where(is1, wt1, 0.0), axis=1, keepdims=True)
                r = pl.ds(pl.multiple_of(j * 128, 128), 128)
                WS[k, r, :] = jnp.broadcast_to(weight, (128, 128))
                PT[k, j] = jnp.transpose(pick).astype(BF16)
                pick = pick.astype(BF16)
                for n in range(4):
                    X[k, r, n * 512 : n * 512 + 512] = dot(
                        pick, T[k, j, :, n * 512 : n * 512 + 512]
                    ).astype(BF16)

    def packed(k):
        sent(f"y{k}")
        sent(f"d{k}")
        pl.semaphore_signal(ready.at[k], inc=1, device_id=sib, device_id_type=MESH)

    def pack_all(k):
        got_all(f"d{k}", T.at[k, :, 128:256])
        pack(k)
        packed(k)

    def gate_up(k, first, last, row=0, rows=512):
        with jax.named_scope(f"gate_up_{k}"):
            @pl.loop(first, last)
            def _(s):
                g = dot(X[k, row : row + rows], W[0, s])
                u = dot(X[k, row : row + rows], W[1, s])
                H[k, s, row : row + rows] = (g / (1.0 + jnp.exp(-g)) * u).astype(BF16)

    here[4].wait()
    with jax.named_scope("attend"):
        attend(0, 2)
    got_all("mz", MT.at[0, 0, 1:4])
    send("myr", MT.at[0, 0], MT.at[0, 3], yr, "my")
    send("myl", MT.at[0, 0], MT.at[0, 1], yl, "my")
    send("myo", MT.at[0, 0], MT.at[0, 2], yo, "my")
    with jax.named_scope("attend"):
        attend(2, 6)
    gather_pass(0)
    gather_start(1)
    gather_start(3)
    send_tile(2)
    got_all("halo", KV.at[:, :, 0 : 2 * WINDOW])
    with jax.named_scope("attend"):
        attend(6, 8)
    got_all("my", MT.at[0, 1:4])
    send("md", MT.at[0], MT.at[1], sib)
    with jax.named_scope("turn"):
        for kp in range(4):
            PMT[kp] = jnp.transpose(PM[kp].astype(F32)).astype(BF16)
    gather_end(0)
    got("md")
    pack_all(0)
    gate_up(0, 0, 1)
    pass_weight(0)
    gather_pass(1)
    gather_start(2)
    gather_pass(3)
    pass_weight(1)
    gather_end(1)
    gate_up(0, 1, 3)
    pack_all(1)
    gate_up(1, 0, 3)
    pass_down(0)
    start_down(1)
    gather_pass(2)
    got("d20", "d23", "d21")
    pack(2, 0, 2)
    pack(2, 3, 4)
    gather_end(3)
    gate_up(2, 0, 3, 0, 256)
    pack_all(3)
    for m in range(2):
        got_all(f"x{m}f", W.at[m, 3])
    gate_up(1, 3, 4)

    def down(c, k):
        with jax.named_scope(f"down_{c}{k}"):
            @pl.loop(0, CHUNKS[c][1] // 256)
            def _(n):
                cols = pl.ds(pl.multiple_of(CHUNKS[c][0] + n * 256, 256), 256)
                out = dot_nt(H[k, 0], W[2, 0, cols, :])
                for s in range(1, 4):
                    out += dot_nt(H[k, s], W[2, s, cols, :])
                scale = WS[k]
                scale = jnp.concatenate([scale, scale], axis=1)
                scaled = (out.astype(BF16).astype(F32) * scale).astype(BF16)
                for j in range(4):
                    part = dot(PT[k, j], scaled[j * 128 : j * 128 + 128])
                    X[k, j * 128 : j * 128 + 128, cols] = part[0:128].astype(BF16)
                    T[k, j, 128:256, cols] = part[128:256].astype(BF16)
        if c == 0:
            pl.semaphore_wait(ready.at[k], 1)
        cols = slice(CHUNKS[c][0], sum(CHUNKS[c]))
        send(f"r{c}{k}", T.at[k, :, 128:256, cols], T.at[k, :, 0:128, cols], sib)

    def plus(c, count, out, *terms):
        step = 16384 // CHUNKS[c][1]

        @pl.loop(0, count // step)
        def _(i):
            r = pl.multiple_of(i * step, step)

            def part(ref, lead, base):
                return (ref, (*lead, pl.ds(base + r, step), slice(CHUNKS[c][0], sum(CHUNKS[c]))))

            total = None
            for term in terms:
                ref, at = part(*term)
                value = ref[at].astype(F32)
                total = value if total is None else total + value
            ref, at = part(*out)
            ref[at] = total.astype(BF16)

    def early(c, k):
        cols = slice(CHUNKS[c][0], sum(CHUNKS[c]))
        got(f"r{c}{k}")
        for j in (2, 1, 3, 0):
            plus(c, 128, (X, (k,), j * 128), (X, (k,), j * 128), (T, (k, j), 0))
            if j == 2:
                send(f"b{c}{k}hr", X.at[k, 256:320, cols], R.at[k, 0, :, cols], yr, f"h{c}{k}", f"b{c}{k}")
                send(f"b{c}{k}hl", X.at[k, 320:384, cols], R.at[k, 1, :, cols], yl, f"h{c}{k}", f"b{c}{k}")
            if j == 1:
                send(f"b{c}{k}er", X.at[k, 192:256, cols], FB.at[k, 0, 64:128, cols], yr, f"F{c}{k}", f"b{c}{k}")
            if j == 3:
                send(f"b{c}{k}el", X.at[k, 384:448, cols], FB.at[k, 1, 0:64, cols], yl, f"F{c}{k}", f"b{c}{k}")

    def late(c, k):
        cols = slice(CHUNKS[c][0], sum(CHUNKS[c]))
        got_all(f"h{c}{k}", R.at[k, :, :, cols])
        plus(c, 64, (X, (k,), 128), (X, (k,), 128), (R, (k, 0), 0))
        send(f"b{c}{k}fr", X.at[k, 128:192, cols], FB.at[k, 0, 0:64, cols], yr, f"F{c}{k}", f"b{c}{k}")
        plus(c, 64, (X, (k,), 448), (X, (k,), 448), (R, (k, 1), 0))
        send(f"b{c}{k}fl", X.at[k, 448:512, cols], FB.at[k, 1, 64:128, cols], yl, f"F{c}{k}", f"b{c}{k}")

    def settle():
        unit, ref = done.pop(0)
        sent("r" + unit)
        sent_all("b" + unit, ref)

    def finish(c, k):
        cols = slice(CHUNKS[c][0], sum(CHUNKS[c]))
        got_all(f"F{c}{k}", FB.at[k, :, :, cols])
        out = (OUT, (0,), 0) if k == 0 else (S, (k - 1,), 0)
        plus(c, 128, out, (X, (k,), 0), (FB, (k, 0), 0), (FB, (k, 1), 0))
        if k:
            send(f"f{c}{k}", S.at[k - 1, :, cols], OUT.at[4 - k, :, cols], zs[k], f"f{c}")

        done.append((f"{c}{k}", X.at[k, 128:512, cols]))
        if len(done) > 1:
            settle()

    homes, done = [], []

    def restore(c):
        got_all(f"f{c}", OUT.at[1:4, :, slice(CHUNKS[c][0], sum(CHUNKS[c]))])
        first, width = CHUNKS[c]
        for piece in range(first // 256, (first + width) // 256):
            cols = slice(piece * 256, piece * 256 + 256)
            spot = (0, piece // 4)
            with jax.named_scope(f"restore_{c}"):
                for half in range(2):
                    total = None
                    for kp in range(4):
                        part = dot(PMT[kp, half * 256 : half * 256 + 256], OUT[kp, :, cols])
                        total = part if total is None else total + part
                    base = piece % 4 * 512 + half * 256
                    W[(*spot, slice(base, base + 256), slice(None))] = total.astype(BF16)
            base = piece % 4 * 512
            homes.append(local(20 + piece, W.at[0, piece // 4, base : base + 512], exp_out.at[:, cols]))

    half_rows = pl.ds(pl.multiple_of(core * 128, 128), 128)

    def start_out():
        here[6].wait()
        send("owr", OW.at[0, half_rows], OW.at[1, half_rows], xr)
        send("owl", OW.at[0, half_rows], OW.at[2, half_rows], xl)
        for name, d, slot, dev in (("ar", 1, 1, xr), ("al", 3, 2, xl), ("ao", 2, 3, xo)):
            part = pl.ds(pl.multiple_of(((tp + d) % 4) * 256, 256), 256)
            send(name, ATT.at[part], AR.at[slot], dev, "a")

    def pass_out():
        low = pl.ds(pl.multiple_of(core * 128, 64), 64)
        high = pl.ds(pl.multiple_of(core * 128 + 64, 64), 64)
        got("owr")
        send("owfr", OW.at[1, low], OW.at[3, low], xr, "owf")
        got("owl")
        send("owfl", OW.at[2, high], OW.at[3, high], xl, "owf")

    def share_out():
        got_all("owf", OW.at[3, half_rows])
        send("owd", OW.at[1:4, half_rows], OW.at[1:4, half_rows], sib)

    def project(half):
        if half == 0:
            got_all("a", AR.at[1:4])
            got("owd")
            here[7].wait()
            AR[0] = ATT[pl.ds(pl.multiple_of(tp * 256, 256), 256), :]
        with jax.named_scope("project"):
            r = slice(half * 128, half * 128 + 128)
            mixed = dot(AR[0, r, :], OW[0])
            for s in range(1, 4):
                mixed += dot(AR[s, r, :], OW[s])
            scale = lax.rsqrt(jnp.mean(mixed * mixed, axis=-1, keepdims=True) + EPS)
            mixed = (mixed * scale * OG[...]).astype(BF16)
            for piece in range(8):
                base = piece * 256 + half * 128
                W[1, 0, base : base + 128] = mixed[:, piece * 256 : piece * 256 + 256]
        if half == 1:
            for piece in range(8):
                base = piece * 256
                homes.append(local(12 + piece, W.at[1, 0, base : base + 256], mix_out.at[:, base : base + 256]))

    hooks = {
        0: [lambda: gate_up(0, 3, 4), lambda: gather_end(2)],
        1: [lambda: pass_down(1), lambda: start_down(2), lambda: gate_up(3, 0, 3)],
        2: [lambda: late(*units[0]), lambda: gate_up(3, 3, 4)],
        3: [lambda: start_down(3), lambda: late(*units[1]), lambda: got("d22"), lambda: pack(2, 2, 3),
            lambda: packed(2), lambda: sent("z")],
        5: [lambda: pass_down(2), lambda: start_down(4), lambda: gate_up(2, 0, 3, 256, 256),
            lambda: gate_up(2, 3, 4)],
        6: [lambda: sent("x"), lambda: sent("m")],
        8: [lambda: pass_down(3)],
        10: [lambda: pass_down(4), start_out],
        13: [lambda: restore(0)],
        14: [pass_out, lambda: sent("w")],
        15: [lambda: restore(1)],
        17: [share_out],
        18: [lambda: restore(2), lambda: project(0)],
        19: [lambda: project(1)],
    }
    units = [(0, 1), (0, 0), (1, 1), (1, 0), (0, 3), (1, 3), (0, 2), (1, 2)]
    units += [(2, 2), (2, 1), (2, 3), (2, 0)]
    units += [(3, 2), (3, 1), (3, 3), (4, 2), (4, 1), (4, 3), (3, 0), (4, 0)]
    count = len(units)
    for i, (c, k) in enumerate(units):
        if all(unit[0] != c for unit in units[:i]):
            first, width = CHUNKS[c]
            got_all(f"w{c}f", W.at[2, 3, first : first + width])
        down(c, k)
        if i >= 1:
            early(*units[i - 1])
        for hook in hooks.get(i, ()):
            hook()
        if i >= 4:
            late(*units[i - 2])
            finish(*units[i - 4])
    early(*units[-1])
    late(*units[-2])
    finish(*units[-4])
    late(*units[-1])
    finish(*units[-3])
    finish(*units[-2])
    restore(3)
    finish(*units[-1])
    restore(4)
    settle()
    sent("")
    assert len(numbers) == COPIES
    with jax.named_scope("home"):
        for copy in homes:
            copy.wait()


def local(
    queries, key_rows, values, sink_logit, out_weight, out_gain, routed_tokens,
    expert_ids, route_weight, routed_gain, expert_gate, expert_up, expert_down,
):
    anywhere = pl.BlockSpec(memory_space=pl.ANY)
    vmem = pl.BlockSpec(memory_space=pltpu.VMEM)
    smem = pl.BlockSpec(memory_space=pltpu.SMEM)
    scratch = [
        pltpu.VMEM((3, 4, 2048, 256), BF16),
        pltpu.VMEM((4, 256, D), BF16),
        pltpu.VMEM((4, 4, 256, D), BF16),
        pltpu.VMEM((4, 512, D), BF16),
        pltpu.VMEM((4, 4, 512, 256), BF16),
        pltpu.VMEM((4, 2, 64, D), BF16),
        pltpu.VMEM((4, 2, 128, D), BF16),
        pltpu.VMEM((3, 128, D), BF16),
        pltpu.VMEM((4, 128, D), BF16),
        pltpu.VMEM((4, 512, 128), F32),
        pltpu.VMEM((4, 4, 256, 128), BF16),
        pltpu.VMEM((4, 128, 512), BF16),
        pltpu.VMEM((4, 512, 128), BF16),
        pltpu.VMEM((2, 4, 4, 16, 128), F32),
        pltpu.VMEM((3, 16, 128), F32),
        pltpu.VMEM((1024, 256), BF16),
        pltpu.VMEM((2, 128, 1024 + 2 * WINDOW), BF16),
        pltpu.VMEM((1024, 256), BF16),
        pltpu.VMEM((4, 256, 256), BF16),
        pltpu.VMEM((1, D), F32),
        pltpu.VMEM((1, D), F32),
        pltpu.SemaphoreType.REGULAR((4,)),
        pltpu.SemaphoreType.DMA((28,)),
        pltpu.SemaphoreType.DMA((SENDS,)),
        pltpu.SemaphoreType.DMA((COPIES,)),
    ]
    return pl.pallas_call(
        kernel,
        out_shape=(
            jax.ShapeDtypeStruct((256, D), BF16),
            jax.ShapeDtypeStruct((512, D), BF16),
        ),
        in_specs=[
            anywhere, anywhere, anywhere, smem, anywhere, anywhere, anywhere, vmem, vmem,
            anywhere, anywhere, anywhere, anywhere,
        ],
        out_specs=(anywhere, anywhere),
        scratch_shapes=scratch,
        compiler_params=pltpu.CompilerParams(
            collective_id=0, has_side_effects=True, vmem_limit_bytes=67043328
        ),
        name="block",
    )(
        queries, key_rows.T, values.T, sink_logit, out_weight, out_gain.reshape(1, D), routed_tokens,
        expert_ids.T, route_weight.T, routed_gain.reshape(1, D), expert_gate.reshape(D, 256),
        expert_up.reshape(D, 256), expert_down.reshape(D, 256),
    )


def solution(mesh):
    placed = (
        P("ep", "tp"), P("ep", "tp"), P("ep", "tp"), P("tp"), P("tp", None), P(),
        P(("ep", "tp"), None), P(("ep", "tp"), None), P(("ep", "tp"), None), P(),
        P("ep", None, "tp"), P("ep", None, "tp"), P("ep", None, "tp"),
    )
    return jax.shard_map(
        local,
        mesh=mesh,
        in_specs=placed,
        out_specs=(P(("ep", "tp"), None), P(("ep", "tp"), None)),
        check_vma=False,
    )
```

```python
import jax
import jax.numpy as jnp
from jax import lax
from jax.experimental import pallas as pl
from jax.experimental.pallas import tpu as pltpu
from jax.sharding import PartitionSpec as P

F32, BF16 = jnp.float32, jnp.bfloat16
MESH = pl.DeviceIdType.MESH
D = 2048
WINDOW = 128
SEQ = 32768
EPS = 1e-06
COPIES = 117
SENDS = 56


def dot(a, b):
    return lax.dot_general(a, b, (((1,), (0,)), ((), ())), preferred_element_type=F32)


def dot_nt(a, b):
    return lax.dot_general(a, b, (((1,), (1,)), ((), ())), preferred_element_type=F32)


def iota(shape, dim):
    return lax.broadcasted_iota(jnp.int32, shape, dim)


CHUNKS = ((0, 256), (256, 256), (512, 512), (1024, 512), (1536, 512))


def kernel(
    q_in, k_in, v_in, sink, ow_in, og_in, tok_in, ids, rw, rg_in, wg_in, wu_in, wd_in,
    mix_out, exp_out,
    W, OW, T, X, H, R, FB, S, OUT, WS, PT, PM, PMT, MT, MS, Q, KV, ATT, AR, OG, RG,
    ready, lsem, ssem, rsem,
):
    ep = lax.axis_index("ep")
    tp = lax.axis_index("tp")
    core, y, z = ep % 2, (ep // 2) % 4, ep // 8

    def place(z, y, core):
        return (z * 4 + y) * 2 + core

    xr, xl, xo = (ep, (tp + 1) % 4), (ep, (tp + 3) % 4), (ep, (tp + 2) % 4)
    yr, yl = (place(z, (y + 1) % 4, core), tp), (place(z, (y + 3) % 4, core), tp)
    yo = (place(z, (y + 2) % 4, core), tp)
    zs = {d: (place((z + d) % 4, y, core), tp) for d in (1, 2, 3)}
    sib = (place(z, y, 1 - core), tp)
    after, before = ((ep + 1) % 32, tp), ((ep + 31) % 32, tp)

    numbers, unsent, copies, groups = {}, {}, {}, {}
    free = list(range(SENDS))[::-1]

    def send(name, src, dst, dev, into=None, group=None):
        if group in groups:
            n = groups[group]
        else:
            n = free.pop()
        copy = pltpu.make_async_remote_copy(
            src_ref=src, dst_ref=dst, send_sem=ssem.at[n],
            recv_sem=rsem.at[numbers.setdefault(into or name, len(numbers))],
            device_id=dev, device_id_type=MESH,
        )
        copy.start()
        assert name not in copies
        copies[name] = copy
        if group:
            groups[group] = n
        else:
            unsent[name] = copy, n

    def got(*names):
        for name in names:
            with jax.named_scope("got_" + name):
                copies[name].wait_recv()

    def whole(ref, n, m):
        return pltpu.make_async_remote_copy(
            src_ref=ref, dst_ref=ref, send_sem=ssem.at[n], recv_sem=rsem.at[m],
            device_id=sib, device_id_type=MESH,
        )

    def got_all(into, ref):
        with jax.named_scope("got_" + into):
            whole(ref, 0, numbers[into]).wait_recv()

    def sent(prefix):
        with jax.named_scope("sent_" + prefix):
            for name in [n for n in unsent if n.startswith(prefix)]:
                copy, n = unsent.pop(name)
                copy.wait_send()
                free.append(n)

    def sent_all(group, ref):
        with jax.named_scope("sent_" + group):
            n = groups.pop(group)
            whole(ref, n, 0).wait_send()
            free.append(n)

    def local(i, src, dst):
        copy = pltpu.make_async_copy(src, dst, lsem.at[i])
        copy.start()
        return copy

    here = [
        local(i, src, dst)
        for i, (src, dst) in enumerate([
            (wg_in, W.at[0, 0]),
            (tok_in, X.at[3]),
            (rg_in, RG),
            (wu_in, W.at[1, 0]),
            (q_in, Q),
            (wd_in, W.at[2, 0]),
            (ow_in, OW.at[0]),
            (og_in, OG),
        ])
    ]
    ours = slice(WINDOW, WINDOW + 1024)
    rows_here = [
        local(8 + 2 * i + half, src, KV.at[i, half * 64 : half * 64 + 64, ours])
        for i, src in enumerate((k_in, v_in))
        for half in range(2)
    ]
    near = (xr, xl, xo, yr, yl, yo, zs[1], zs[2], zs[3], sib, after, before)
    barrier = pltpu.get_barrier_semaphore()
    for dev in near:
        pl.semaphore_signal(barrier, inc=1, device_id=dev, device_id_type=MESH)

    def pass_weight(m):
        got(f"x{m}r")
        send(f"x{m}fr", W.at[m, 1, 0:1024], W.at[m, 3, 0:1024], xr, f"x{m}f")
        got(f"x{m}l")
        send(f"x{m}fl", W.at[m, 2, 1024:2048], W.at[m, 3, 1024:2048], xl, f"x{m}f")

    def start_down(c):
        rows = slice(CHUNKS[c][0], sum(CHUNKS[c]))
        send(f"w{c}r", W.at[2, 0, rows], W.at[2, 1, rows], xr)
        send(f"w{c}l", W.at[2, 0, rows], W.at[2, 2, rows], xl)

    def pass_down(c):
        first, width = CHUNKS[c]
        low, high = slice(first, first + width // 2), slice(first + width // 2, first + width)
        got(f"w{c}r")
        send(f"w{c}fr", W.at[2, 1, low], W.at[2, 3, low], xr, f"w{c}f")
        got(f"w{c}l")
        send(f"w{c}fl", W.at[2, 2, high], W.at[2, 3, high], xl, f"w{c}f")

    with jax.named_scope("routing"):
        id0, id1 = ids[0:1, :].astype(F32), ids[1:2, :].astype(F32)
        w0, w1 = rw[0:1, :], rw[1:2, :]
        ie = iota((32, 512), 0).astype(F32)
        one0 = jnp.where(ie == id0, 1.0, 0.0)
        one1 = jnp.where(ie == id1, 1.0, 0.0)
        upper = jnp.where(iota((512, 512), 0) < iota((512, 512), 1), 1.0, 0.0).astype(BF16)
        ahead = dot((one0 + one1).astype(BF16), upper)
        slot0 = jnp.sum(ahead * one0, axis=0, keepdims=True)
        slot1 = jnp.sum(ahead * one1, axis=0, keepdims=True) + jnp.where(id0 == id1, 1.0, 0.0)
        gid = jnp.floor(id0 * 0.125)
        oneg = jnp.where(iota((8, 512), 0).astype(F32) == gid, 1.0, 0.0)
        rank = jnp.sum(dot(oneg.astype(BF16), upper) * oneg, axis=0, keepdims=True)
        dest = gid * 128.0 + rank

        def split(w):
            high = w.astype(BF16).astype(F32)
            mid = (w - high).astype(BF16).astype(F32)
            return high, mid, w - high - mid

        rows16 = iota((16, 512), 0)
        m16 = jnp.zeros((16, 512), F32)
        for i, row in enumerate((id0, slot0, id1, slot1, *split(w0), *split(w1))):
            m16 = jnp.where(rows16 == i, row, m16)
        m16 = m16.astype(BF16)
        for kp in range(4):
            base = ((z + kp) % 4) * 128
            pm = jnp.where((iota((128, 512), 0) + base).astype(F32) == dest, 1.0, 0.0)
            PM[kp] = pm.astype(BF16)
            moved = dot_nt(m16, pm.astype(BF16))
            if kp == 0:
                MT[0, 0, 0] = moved
            else:
                MS[kp - 1] = moved
    with jax.named_scope("barrier"):
        pl.semaphore_wait(barrier, len(near))

    def start_weight(m, copy):
        copy.wait()
        send(f"x{m}r", W.at[m, 0], W.at[m, 1], xr)
        send(f"x{m}l", W.at[m, 0], W.at[m, 2], xl)

    start_weight(0, here[0])
    here[1].wait()
    here[2].wait()
    def shared(k):
        return None if k == 2 else f"d{k}"

    def start_tile(k):
        send(f"y{k}r", T.at[k, 0, 0:128], T.at[k, 3, 0:128], yr)
        send(f"y{k}l", T.at[k, 0, 0:128], T.at[k, 1, 0:128], yl)
        send(f"d{k}0", T.at[k, 0, 0:128], T.at[k, 0, 128:256], sib, shared(k))

    def permute(kp):
        with jax.named_scope(f"permute_{kp}"):
            v = dot(PM[kp], X[3])
            scale = lax.rsqrt(jnp.mean(v * v, axis=-1, keepdims=True) + EPS)
            tile = (v * scale * RG[...]).astype(BF16)
            if kp == 0:
                T[0, 0, 0:128] = tile
            else:
                S[kp - 1] = tile

    def send_tile(kp):
        send(f"z{kp}", S.at[kp - 1], T.at[4 - kp, 0, 0:128], zs[kp])

    permute(0)
    for kp in (1, 3, 2):
        send(f"mz{kp}", MS.at[kp - 1], MT.at[0, 0, 4 - kp], zs[kp], "mz")
    for copy in rows_here:
        copy.wait()
    send("halo_n", KV.at[:, :, 1024 : 1024 + WINDOW], KV.at[:, :, 0:WINDOW], after, "halo")
    send("halo_p", KV.at[:, :, WINDOW : 2 * WINDOW], KV.at[:, :, 1024 + WINDOW :], before, "halo")
    start_tile(0)
    start_weight(1, here[3])
    here[5].wait()
    start_down(0)
    for kp in (1, 3):
        permute(kp)
        send_tile(kp)
    permute(2)

    def gather_start(k):
        got(f"z{4 - k}")
        start_tile(k)

    def gather_pass(k):
        got(f"y{k}r")
        send(f"y{k}fr", T.at[k, 3, 0:64], T.at[k, 2, 0:64], yr, f"y{k}f")
        send(f"d{k}3", T.at[k, 3, 0:128], T.at[k, 3, 128:256], sib, shared(k))
        got(f"y{k}l")
        send(f"y{k}fl", T.at[k, 1, 64:128], T.at[k, 2, 64:128], yl, f"y{k}f")
        send(f"d{k}1", T.at[k, 1, 0:128], T.at[k, 1, 128:256], sib, shared(k))

    def gather_end(k):
        got_all(f"y{k}f", T.at[k, 2, 0:128])
        send(f"d{k}2", T.at[k, 2, 0:128], T.at[k, 2, 128:256], sib, shared(k))

    def attend(first, last):
        lane = iota((128, 128), 1)
        c_pos = iota((128, 384), 1)
        gap = c_pos - iota((128, 384), 0)

        @pl.loop(first, last)
        def _(i):
            b = (i + 1) % 8
            r0 = pl.multiple_of(b * 128, 128)
            kk = KV[0, :, pl.ds(r0, 384)]
            vv = KV[1, :, pl.ds(r0, 384)]
            key = c_pos + (ep * 1024 + b * 128 - WINDOW)
            valid = (gap >= 0) & (gap <= 2 * WINDOW) & (key >= 0) & (key < SEQ)
            found = []
            for h in range(4):
                qh = Q[pl.ds(r0, 128), (h // 2) * 128 : (h // 2) * 128 + 128]
                qh = jnp.where((lane < 64) if h % 2 == 0 else (lane >= 64), qh, 0.0).astype(BF16)
                s = dot(qh, kk) * 0.125
                s = jnp.where(valid, s, -1e30)
                largest = jnp.maximum(jnp.max(s, axis=-1, keepdims=True), sink[h])
                e = jnp.where(valid, jnp.exp(s - largest), 0.0)
                total = jnp.sum(e, axis=-1, keepdims=True) + jnp.exp(sink[h] - largest)
                found.append(dot_nt((e / total).astype(BF16), vv))
            ATT[pl.ds(r0, 128), 0:128] = jnp.where(lane < 64, found[0], found[1]).astype(BF16)
            ATT[pl.ds(r0, 128), 128:256] = jnp.where(lane < 64, found[2], found[3]).astype(BF16)

    me = ep.astype(F32)

    def pack(k, first=0, last=4):
        with jax.named_scope(f"pack_{k}"):
            @pl.loop(first, last)
            def _(j):
                both = jnp.concatenate([MT[0, j, k], MT[1, j, k]], axis=1)
                shift = jnp.where(iota((1, 256), 1) >= 128, 64.0, 0.0)
                sl0 = jnp.where(both[0:1] == me, both[1:2] + shift, -1.0)
                sl1 = jnp.where(both[2:3] == me, both[3:4] + shift, -1.0)
                wt0 = both[4:5] + both[5:6] + both[6:7]
                wt1 = both[7:8] + both[8:9] + both[9:10]
                rows = iota((128, 256), 0).astype(F32)
                is0, is1 = rows == sl0, rows == sl1
                pick = jnp.where(is0 | is1, 1.0, 0.0)
                weight = jnp.sum(jnp.where(is0, wt0, 0.0) + jnp.where(is1, wt1, 0.0), axis=1, keepdims=True)
                r = pl.ds(pl.multiple_of(j * 128, 128), 128)
                WS[k, r, :] = jnp.broadcast_to(weight, (128, 128))
                PT[k, j] = jnp.transpose(pick).astype(BF16)
                pick = pick.astype(BF16)
                for n in range(4):
                    X[k, r, n * 512 : n * 512 + 512] = dot(
                        pick, T[k, j, :, n * 512 : n * 512 + 512]
                    ).astype(BF16)

    def packed(k):
        sent(f"y{k}")
        sent(f"d{k}")
        pl.semaphore_signal(ready.at[k], inc=1, device_id=sib, device_id_type=MESH)

    def pack_all(k):
        got_all(f"d{k}", T.at[k, :, 128:256])
        pack(k)
        packed(k)

    def gate_up(k, first, last, row=0, rows=512):
        with jax.named_scope(f"gate_up_{k}"):
            @pl.loop(first, last)
            def _(s):
                g = dot(X[k, row : row + rows], W[0, s])
                u = dot(X[k, row : row + rows], W[1, s])
                H[k, s, row : row + rows] = (g / (1.0 + jnp.exp(-g)) * u).astype(BF16)

    here[4].wait()
    with jax.named_scope("attend"):
        attend(0, 2)
    got_all("mz", MT.at[0, 0, 1:4])
    send("myr", MT.at[0, 0], MT.at[0, 3], yr, "my")
    send("myl", MT.at[0, 0], MT.at[0, 1], yl, "my")
    send("myo", MT.at[0, 0], MT.at[0, 2], yo, "my")
    with jax.named_scope("attend"):
        attend(2, 6)
    gather_pass(0)
    gather_start(1)
    gather_start(3)
    send_tile(2)
    got_all("halo", KV.at[:, :, 0 : 2 * WINDOW])
    with jax.named_scope("attend"):
        attend(6, 8)
    got_all("my", MT.at[0, 1:4])
    send("md", MT.at[0], MT.at[1], sib)
    with jax.named_scope("turn"):
        for kp in range(4):
            PMT[kp] = jnp.transpose(PM[kp].astype(F32)).astype(BF16)
    gather_end(0)
    got("md")
    pack_all(0)
    gate_up(0, 0, 1)
    pass_weight(0)
    gather_pass(1)
    gather_start(2)
    gather_pass(3)
    pass_weight(1)
    gather_end(1)
    gate_up(0, 1, 3)
    pack_all(1)
    gate_up(1, 0, 3)
    pass_down(0)
    start_down(1)
    start_down(2)
    gather_pass(2)
    got("d20", "d23", "d21")
    pack(2, 0, 2)
    pack(2, 3, 4)
    gate_up(2, 0, 3, 0, 256)
    gather_end(3)
    gate_up(2, 0, 3, 384, 128)
    pack_all(3)
    gate_up(3, 0, 3)
    for m in range(2):
        got_all(f"x{m}f", W.at[m, 3])
    gate_up(1, 3, 4)

    def down(c, k):
        with jax.named_scope(f"down_{c}{k}"):
            @pl.loop(0, CHUNKS[c][1] // 256)
            def _(n):
                cols = pl.ds(pl.multiple_of(CHUNKS[c][0] + n * 256, 256), 256)
                out = dot_nt(H[k, 0], W[2, 0, cols, :])
                for s in range(1, 4):
                    out += dot_nt(H[k, s], W[2, s, cols, :])
                scale = WS[k]
                scale = jnp.concatenate([scale, scale], axis=1)
                scaled = (out.astype(BF16).astype(F32) * scale).astype(BF16)
                for j in range(4):
                    part = dot(PT[k, j], scaled[j * 128 : j * 128 + 128])
                    X[k, j * 128 : j * 128 + 128, cols] = part[0:128].astype(BF16)
                    T[k, j, 128:256, cols] = part[128:256].astype(BF16)
        if c == 0:
            pl.semaphore_wait(ready.at[k], 1)
        cols = slice(CHUNKS[c][0], sum(CHUNKS[c]))
        send(f"r{c}{k}", T.at[k, :, 128:256, cols], T.at[k, :, 0:128, cols], sib)

    def plus(c, count, out, *terms):
        step = 16384 // CHUNKS[c][1]

        @pl.loop(0, count // step)
        def _(i):
            r = pl.multiple_of(i * step, step)

            def part(ref, lead, base):
                return (ref, (*lead, pl.ds(base + r, step), slice(CHUNKS[c][0], sum(CHUNKS[c]))))

            total = None
            for term in terms:
                ref, at = part(*term)
                value = ref[at].astype(F32)
                total = value if total is None else total + value
            ref, at = part(*out)
            ref[at] = total.astype(BF16)

    def early(c, k):
        cols = slice(CHUNKS[c][0], sum(CHUNKS[c]))
        got(f"r{c}{k}")
        for j in (2, 1, 3, 0):
            plus(c, 128, (X, (k,), j * 128), (X, (k,), j * 128), (T, (k, j), 0))
            if j == 2:
                send(f"b{c}{k}hr", X.at[k, 256:320, cols], R.at[k, 0, :, cols], yr, f"h{c}{k}", f"b{c}{k}")
                send(f"b{c}{k}hl", X.at[k, 320:384, cols], R.at[k, 1, :, cols], yl, f"h{c}{k}", f"b{c}{k}")
            if j == 1:
                send(f"b{c}{k}er", X.at[k, 192:256, cols], FB.at[k, 0, 64:128, cols], yr, f"F{c}{k}", f"b{c}{k}")
            if j == 3:
                send(f"b{c}{k}el", X.at[k, 384:448, cols], FB.at[k, 1, 0:64, cols], yl, f"F{c}{k}", f"b{c}{k}")

    def late(c, k):
        cols = slice(CHUNKS[c][0], sum(CHUNKS[c]))
        got_all(f"h{c}{k}", R.at[k, :, :, cols])
        plus(c, 64, (X, (k,), 128), (X, (k,), 128), (R, (k, 0), 0))
        send(f"b{c}{k}fr", X.at[k, 128:192, cols], FB.at[k, 0, 0:64, cols], yr, f"F{c}{k}", f"b{c}{k}")
        plus(c, 64, (X, (k,), 448), (X, (k,), 448), (R, (k, 1), 0))
        send(f"b{c}{k}fl", X.at[k, 448:512, cols], FB.at[k, 1, 64:128, cols], yl, f"F{c}{k}", f"b{c}{k}")

    def settle():
        unit, ref = done.pop(0)
        sent("r" + unit)
        sent_all("b" + unit, ref)

    def finish(c, k):
        cols = slice(CHUNKS[c][0], sum(CHUNKS[c]))
        got_all(f"F{c}{k}", FB.at[k, :, :, cols])
        out = (OUT, (0,), 0) if k == 0 else (S, (k - 1,), 0)
        plus(c, 128, out, (X, (k,), 0), (FB, (k, 0), 0), (FB, (k, 1), 0))
        if k:
            send(f"f{c}{k}", S.at[k - 1, :, cols], OUT.at[4 - k, :, cols], zs[k], f"f{c}")

        done.append((f"{c}{k}", X.at[k, 128:512, cols]))
        if len(done) > 1:
            settle()

    homes, done = [], []

    def restore(c):
        got_all(f"f{c}", OUT.at[1:4, :, slice(CHUNKS[c][0], sum(CHUNKS[c]))])
        first, width = CHUNKS[c]
        for piece in range(first // 256, (first + width) // 256):
            cols = slice(piece * 256, piece * 256 + 256)
            spot = (0, piece // 4)
            with jax.named_scope(f"restore_{c}"):
                for half in range(2):
                    total = None
                    for kp in range(4):
                        part = dot(PMT[kp, half * 256 : half * 256 + 256], OUT[kp, :, cols])
                        total = part if total is None else total + part
                    base = piece % 4 * 512 + half * 256
                    W[(*spot, slice(base, base + 256), slice(None))] = total.astype(BF16)
            base = piece % 4 * 512
            homes.append(local(20 + piece, W.at[0, piece // 4, base : base + 512], exp_out.at[:, cols]))

    half_rows = pl.ds(pl.multiple_of(core * 128, 128), 128)

    def start_out():
        here[6].wait()
        send("owr", OW.at[0, half_rows], OW.at[1, half_rows], xr)
        send("owl", OW.at[0, half_rows], OW.at[2, half_rows], xl)
        for name, d, slot, dev in (("ar", 1, 1, xr), ("al", 3, 2, xl), ("ao", 2, 3, xo)):
            part = pl.ds(pl.multiple_of(((tp + d) % 4) * 256, 256), 256)
            send(name, ATT.at[part], AR.at[slot], dev, "a")

    def pass_out():
        low = pl.ds(pl.multiple_of(core * 128, 64), 64)
        high = pl.ds(pl.multiple_of(core * 128 + 64, 64), 64)
        got("owr")
        send("owfr", OW.at[1, low], OW.at[3, low], xr, "owf")
        got("owl")
        send("owfl", OW.at[2, high], OW.at[3, high], xl, "owf")

    def share_out():
        got_all("owf", OW.at[3, half_rows])
        send("owd", OW.at[1:4, half_rows], OW.at[1:4, half_rows], sib)

    def project(half):
        if half == 0:
            got_all("a", AR.at[1:4])
            got("owd")
            here[7].wait()
            AR[0] = ATT[pl.ds(pl.multiple_of(tp * 256, 256), 256), :]
        with jax.named_scope("project"):
            r = slice(half * 128, half * 128 + 128)
            mixed = dot(AR[0, r, :], OW[0])
            for s in range(1, 4):
                mixed += dot(AR[s, r, :], OW[s])
            scale = lax.rsqrt(jnp.mean(mixed * mixed, axis=-1, keepdims=True) + EPS)
            mixed = (mixed * scale * OG[...]).astype(BF16)
            for piece in range(8):
                base = piece * 256 + half * 128
                W[1, 0, base : base + 128] = mixed[:, piece * 256 : piece * 256 + 256]
        if half == 1:
            for piece in range(8):
                base = piece * 256
                homes.append(local(12 + piece, W.at[1, 0, base : base + 256], mix_out.at[:, base : base + 256]))

    units = [(c, k) for c in range(2) for k in (1, 0, 3, 2)]
    units += [(2, 2), (2, 1), (2, 3), (2, 0)]
    units += [(3, 2), (3, 1), (3, 3), (4, 2), (4, 1), (4, 3), (3, 0), (4, 0)]
    arrived = set()

    def produce(i):
        c, k = units[i]
        if c not in arrived:
            arrived.add(c)
            first, width = CHUNKS[c]
            got_all(f"w{c}f", W.at[2, 3, first : first + width])
        down(c, k)

    produce(0)
    gate_up(0, 3, 4)
    gather_end(2)
    produce(1)
    pass_down(1)
    early(*units[0])
    gate_up(3, 3, 4)
    early(*units[1])
    produce(2)
    got("d22")
    pack(2, 2, 3)
    packed(2)
    gate_up(2, 0, 3, 256, 128)
    early(*units[2])
    pass_down(2)
    start_down(3)
    start_down(4)
    gate_up(2, 3, 4)
    produce(3)
    late(*units[0])
    sent("z")

    hooks = {
        6: [lambda: sent("x"), lambda: sent("m")],
        9: [lambda: pass_down(3)],
        10: [lambda: pass_down(4), start_out],
        13: [lambda: restore(0)],
        15: [pass_out, lambda: sent("w"), lambda: restore(1)],
        17: [share_out],
        18: [lambda: restore(2)],
        19: [lambda: project(0)],
    }
    passed, ended = 1, 0
    for i in range(4, len(units)):
        produce(i)
        early(*units[i - 1])
        for hook in hooks.get(i, ()):
            hook()
        lag = 4 if i < 9 else 3 if i < 12 else 2
        while passed <= i - lag:
            late(*units[passed])
            passed += 1
        while ended <= i - lag - 3:
            finish(*units[ended])
            ended += 1
    early(*units[-1])
    project(1)
    finish(*units[-5])
    late(*units[-2])
    finish(*units[-4])
    late(*units[-1])
    finish(*units[-3])
    finish(*units[-2])
    restore(3)
    finish(*units[-1])
    restore(4)
    settle()
    sent("")
    assert len(numbers) == COPIES
    with jax.named_scope("home"):
        for copy in homes:
            copy.wait()


def local(
    queries, key_rows, values, sink_logit, out_weight, out_gain, routed_tokens,
    expert_ids, route_weight, routed_gain, expert_gate, expert_up, expert_down,
):
    anywhere = pl.BlockSpec(memory_space=pl.ANY)
    vmem = pl.BlockSpec(memory_space=pltpu.VMEM)
    smem = pl.BlockSpec(memory_space=pltpu.SMEM)
    scratch = [
        pltpu.VMEM((3, 4, 2048, 256), BF16),
        pltpu.VMEM((4, 256, D), BF16),
        pltpu.VMEM((4, 4, 256, D), BF16),
        pltpu.VMEM((4, 512, D), BF16),
        pltpu.VMEM((4, 4, 512, 256), BF16),
        pltpu.VMEM((4, 2, 64, D), BF16),
        pltpu.VMEM((4, 2, 128, D), BF16),
        pltpu.VMEM((3, 128, D), BF16),
        pltpu.VMEM((4, 128, D), BF16),
        pltpu.VMEM((4, 512, 128), F32),
        pltpu.VMEM((4, 4, 256, 128), BF16),
        pltpu.VMEM((4, 128, 512), BF16),
        pltpu.VMEM((4, 512, 128), BF16),
        pltpu.VMEM((2, 4, 4, 16, 128), F32),
        pltpu.VMEM((3, 16, 128), F32),
        pltpu.VMEM((1024, 256), BF16),
        pltpu.VMEM((2, 128, 1024 + 2 * WINDOW), BF16),
        pltpu.VMEM((1024, 256), BF16),
        pltpu.VMEM((4, 256, 256), BF16),
        pltpu.VMEM((1, D), F32),
        pltpu.VMEM((1, D), F32),
        pltpu.SemaphoreType.REGULAR((4,)),
        pltpu.SemaphoreType.DMA((28,)),
        pltpu.SemaphoreType.DMA((SENDS,)),
        pltpu.SemaphoreType.DMA((COPIES,)),
    ]
    return pl.pallas_call(
        kernel,
        out_shape=(
            jax.ShapeDtypeStruct((256, D), BF16),
            jax.ShapeDtypeStruct((512, D), BF16),
        ),
        in_specs=[
            anywhere, anywhere, anywhere, smem, anywhere, anywhere, anywhere, vmem, vmem,
            anywhere, anywhere, anywhere, anywhere,
        ],
        out_specs=(anywhere, anywhere),
        scratch_shapes=scratch,
        compiler_params=pltpu.CompilerParams(
            collective_id=0, has_side_effects=True, vmem_limit_bytes=67043328
        ),
        name="block",
    )(
        queries, key_rows.T, values.T, sink_logit, out_weight, out_gain.reshape(1, D), routed_tokens,
        expert_ids.T, route_weight.T, routed_gain.reshape(1, D), expert_gate.reshape(D, 256),
        expert_up.reshape(D, 256), expert_down.reshape(D, 256),
    )


def solution(mesh):
    placed = (
        P("ep", "tp"), P("ep", "tp"), P("ep", "tp"), P("tp"), P("tp", None), P(),
        P(("ep", "tp"), None), P(("ep", "tp"), None), P(("ep", "tp"), None), P(),
        P("ep", None, "tp"), P("ep", None, "tp"), P("ep", None, "tp"),
    )
    return jax.shard_map(
        local,
        mesh=mesh,
        in_specs=placed,
        out_specs=(P(("ep", "tp"), None), P(("ep", "tp"), None)),
        check_vma=False,
    )
```

```python
import jax
import jax.numpy as jnp
from jax import lax
from jax.experimental import pallas as pl
from jax.experimental.pallas import tpu as pltpu
from jax.sharding import PartitionSpec as P

F32, BF16 = jnp.float32, jnp.bfloat16
MESH = pl.DeviceIdType.MESH
D = 2048
WINDOW = 128
SEQ = 32768
EPS = 1e-06
COPIES = 119
SENDS = 56


def dot(a, b):
    return lax.dot_general(a, b, (((1,), (0,)), ((), ())), preferred_element_type=F32)


def dot_nt(a, b):
    return lax.dot_general(a, b, (((1,), (1,)), ((), ())), preferred_element_type=F32)


def iota(shape, dim):
    return lax.broadcasted_iota(jnp.int32, shape, dim)


CHUNKS = ((0, 256), (256, 256), (512, 512), (1024, 512), (1536, 512))


def kernel(
    q_in, k_in, v_in, sink, ow_in, og_in, tok_in, ids, rw, rg_in, wg_in, wu_in, wd_in,
    mix_out, exp_out,
    W, OW, T, X, H, R, FB, S, OUT, WS, PT, PM, PMT, MT, MS, Q, KV, ATT, AR, OG, RG,
    ready, lsem, ssem, rsem,
):
    ep = lax.axis_index("ep")
    tp = lax.axis_index("tp")
    core, y, z = ep % 2, (ep // 2) % 4, ep // 8

    def place(z, y, core):
        return (z * 4 + y) * 2 + core

    xr, xl, xo = (ep, (tp + 1) % 4), (ep, (tp + 3) % 4), (ep, (tp + 2) % 4)
    yr, yl = (place(z, (y + 1) % 4, core), tp), (place(z, (y + 3) % 4, core), tp)
    yo = (place(z, (y + 2) % 4, core), tp)
    zs = {d: (place((z + d) % 4, y, core), tp) for d in (1, 2, 3)}
    sib = (place(z, y, 1 - core), tp)
    after, before = ((ep + 1) % 32, tp), ((ep + 31) % 32, tp)

    numbers, unsent, copies, groups = {}, {}, {}, {}
    free = list(range(SENDS))[::-1]

    def send(name, src, dst, dev, into=None, group=None):
        if group in groups:
            n = groups[group]
        else:
            n = free.pop()
        copy = pltpu.make_async_remote_copy(
            src_ref=src, dst_ref=dst, send_sem=ssem.at[n],
            recv_sem=rsem.at[numbers.setdefault(into or name, len(numbers))],
            device_id=dev, device_id_type=MESH,
        )
        copy.start()
        assert name not in copies
        copies[name] = copy
        if group:
            groups[group] = n
        else:
            unsent[name] = copy, n

    def got(*names):
        for name in names:
            with jax.named_scope("got_" + name):
                copies[name].wait_recv()

    def whole(ref, n, m):
        return pltpu.make_async_remote_copy(
            src_ref=ref, dst_ref=ref, send_sem=ssem.at[n], recv_sem=rsem.at[m],
            device_id=sib, device_id_type=MESH,
        )

    def got_all(into, ref):
        with jax.named_scope("got_" + into):
            whole(ref, 0, numbers[into]).wait_recv()

    def sent(prefix):
        with jax.named_scope("sent_" + prefix):
            for name in [n for n in unsent if n.startswith(prefix)]:
                copy, n = unsent.pop(name)
                copy.wait_send()
                free.append(n)

    def sent_all(group, ref):
        with jax.named_scope("sent_" + group):
            n = groups.pop(group)
            whole(ref, n, 0).wait_send()
            free.append(n)

    def local(i, src, dst):
        copy = pltpu.make_async_copy(src, dst, lsem.at[i])
        copy.start()
        return copy

    here = [
        local(i, src, dst)
        for i, (src, dst) in enumerate([
            (wg_in, W.at[0, 0]),
            (tok_in, X.at[3]),
            (rg_in, RG),
            (wu_in, W.at[1, 0]),
            (q_in, Q),
            (wd_in, W.at[2, 0]),
            (ow_in, OW.at[0]),
            (og_in, OG),
        ])
    ]
    ours = slice(WINDOW, WINDOW + 1024)
    rows_here = [
        local(8 + 2 * i + half, src, KV.at[i, half * 64 : half * 64 + 64, ours])
        for i, src in enumerate((k_in, v_in))
        for half in range(2)
    ]
    near = (xr, xl, xo, yr, yl, yo, zs[1], zs[2], zs[3], sib, after, before)
    barrier = pltpu.get_barrier_semaphore()
    for dev in near:
        pl.semaphore_signal(barrier, inc=1, device_id=dev, device_id_type=MESH)

    def pass_weight(m):
        got(f"x{m}r")
        send(f"x{m}fr", W.at[m, 1, 0:1024], W.at[m, 3, 0:1024], xr, f"x{m}f")
        got(f"x{m}l")
        send(f"x{m}fl", W.at[m, 2, 1024:2048], W.at[m, 3, 1024:2048], xl, f"x{m}f")

    def start_down(c):
        rows = slice(CHUNKS[c][0], sum(CHUNKS[c]))
        send(f"w{c}r", W.at[2, 0, rows], W.at[2, 1, rows], xr)
        send(f"w{c}l", W.at[2, 0, rows], W.at[2, 2, rows], xl)

    def pass_down(c):
        first, width = CHUNKS[c]
        low, high = slice(first, first + width // 2), slice(first + width // 2, first + width)
        got(f"w{c}r")
        send(f"w{c}fr", W.at[2, 1, low], W.at[2, 3, low], xr, f"w{c}f")
        got(f"w{c}l")
        send(f"w{c}fl", W.at[2, 2, high], W.at[2, 3, high], xl, f"w{c}f")

    with jax.named_scope("routing"):
        id0, id1 = ids[0:1, :].astype(F32), ids[1:2, :].astype(F32)
        w0, w1 = rw[0:1, :], rw[1:2, :]
        ie = iota((32, 512), 0).astype(F32)
        one0 = jnp.where(ie == id0, 1.0, 0.0)
        one1 = jnp.where(ie == id1, 1.0, 0.0)
        upper = jnp.where(iota((512, 512), 0) < iota((512, 512), 1), 1.0, 0.0).astype(BF16)
        ahead = dot((one0 + one1).astype(BF16), upper)
        slot0 = jnp.sum(ahead * one0, axis=0, keepdims=True)
        slot1 = jnp.sum(ahead * one1, axis=0, keepdims=True) + jnp.where(id0 == id1, 1.0, 0.0)
        gid = jnp.floor(id0 * 0.125)
        oneg = jnp.where(iota((8, 512), 0).astype(F32) == gid, 1.0, 0.0)
        rank = jnp.sum(dot(oneg.astype(BF16), upper) * oneg, axis=0, keepdims=True)
        dest = gid * 128.0 + rank

        def split(w):
            high = w.astype(BF16).astype(F32)
            mid = (w - high).astype(BF16).astype(F32)
            return high, mid, w - high - mid

        rows16 = iota((16, 512), 0)
        m16 = jnp.zeros((16, 512), F32)
        for i, row in enumerate((id0, slot0, id1, slot1, *split(w0), *split(w1))):
            m16 = jnp.where(rows16 == i, row, m16)
        m16 = m16.astype(BF16)
        for kp in range(4):
            base = ((z + kp) % 4) * 128
            pm = jnp.where((iota((128, 512), 0) + base).astype(F32) == dest, 1.0, 0.0)
            PM[kp] = pm.astype(BF16)
            moved = dot_nt(m16, pm.astype(BF16))
            if kp == 0:
                MT[0, 0, 0] = moved
            else:
                MS[kp - 1] = moved
    with jax.named_scope("barrier"):
        pl.semaphore_wait(barrier, len(near))

    def start_weight(m, copy):
        copy.wait()
        send(f"x{m}r", W.at[m, 0], W.at[m, 1], xr)
        send(f"x{m}l", W.at[m, 0], W.at[m, 2], xl)

    start_weight(0, here[0])
    here[1].wait()
    here[2].wait()
    def shared(k):
        return None if k == 2 else f"d{k}"

    def start_tile(k):
        send(f"y{k}r", T.at[k, 0, 0:128], T.at[k, 3, 0:128], yr)
        send(f"y{k}l", T.at[k, 0, 0:128], T.at[k, 1, 0:128], yl)
        send(f"d{k}0", T.at[k, 0, 0:128], T.at[k, 0, 128:256], sib, shared(k))

    def permute(kp):
        with jax.named_scope(f"permute_{kp}"):
            v = dot(PM[kp], X[3])
            scale = lax.rsqrt(jnp.mean(v * v, axis=-1, keepdims=True) + EPS)
            tile = (v * scale * RG[...]).astype(BF16)
            if kp == 0:
                T[0, 0, 0:128] = tile
            else:
                S[kp - 1] = tile

    def send_tile(kp):
        send(f"z{kp}", S.at[kp - 1], T.at[4 - kp, 0, 0:128], zs[kp])

    permute(0)
    for kp in (1, 3, 2):
        send(f"mz{kp}", MS.at[kp - 1], MT.at[0, 0, 4 - kp], zs[kp], "mz")
    for copy in rows_here:
        copy.wait()
    send("halo_n", KV.at[:, :, 1024 : 1024 + WINDOW], KV.at[:, :, 0:WINDOW], after, "halo")
    send("halo_p", KV.at[:, :, WINDOW : 2 * WINDOW], KV.at[:, :, 1024 + WINDOW :], before, "halo")
    for name, j, dev, halves in (("r", 3, yr, (0, 64)), ("l", 1, yl, (64, 0))):
        for part, row in zip("ab", halves):
            rows = slice(row, row + 64)
            send(f"y0{name}{part}", T.at[0, 0, rows], T.at[0, j, rows], dev)
    send("d00", T.at[0, 0, 0:128], T.at[0, 0, 128:256], sib, "d0")
    start_weight(1, here[3])
    here[5].wait()
    start_down(0)
    for kp in (1, 3):
        permute(kp)
        send_tile(kp)
    permute(2)

    def gather_start(k):
        got(f"z{4 - k}")
        start_tile(k)

    def gather_pass(k):
        got(f"y{k}r")
        send(f"y{k}fr", T.at[k, 3, 0:64], T.at[k, 2, 0:64], yr, f"y{k}f")
        send(f"d{k}3", T.at[k, 3, 0:128], T.at[k, 3, 128:256], sib, shared(k))
        got(f"y{k}l")
        send(f"y{k}fl", T.at[k, 1, 64:128], T.at[k, 2, 64:128], yl, f"y{k}f")
        send(f"d{k}1", T.at[k, 1, 0:128], T.at[k, 1, 128:256], sib, shared(k))

    def gather_end(k):
        got_all(f"y{k}f", T.at[k, 2, 0:128])
        send(f"d{k}2", T.at[k, 2, 0:128], T.at[k, 2, 128:256], sib, shared(k))

    def attend(first, last):
        lane = iota((128, 128), 1)
        c_pos = iota((128, 384), 1)
        gap = c_pos - iota((128, 384), 0)

        @pl.loop(first, last)
        def _(i):
            b = (i + 1) % 8
            r0 = pl.multiple_of(b * 128, 128)
            kk = KV[0, :, pl.ds(r0, 384)]
            vv = KV[1, :, pl.ds(r0, 384)]
            key = c_pos + (ep * 1024 + b * 128 - WINDOW)
            valid = (gap >= 0) & (gap <= 2 * WINDOW) & (key >= 0) & (key < SEQ)
            found = []
            for h in range(4):
                qh = Q[pl.ds(r0, 128), (h // 2) * 128 : (h // 2) * 128 + 128]
                qh = jnp.where((lane < 64) if h % 2 == 0 else (lane >= 64), qh, 0.0).astype(BF16)
                s = dot(qh, kk) * 0.125
                s = jnp.where(valid, s, -1e30)
                largest = jnp.maximum(jnp.max(s, axis=-1, keepdims=True), sink[h])
                e = jnp.where(valid, jnp.exp(s - largest), 0.0)
                total = jnp.sum(e, axis=-1, keepdims=True) + jnp.exp(sink[h] - largest)
                found.append(dot_nt((e / total).astype(BF16), vv))
            ATT[pl.ds(r0, 128), 0:128] = jnp.where(lane < 64, found[0], found[1]).astype(BF16)
            ATT[pl.ds(r0, 128), 128:256] = jnp.where(lane < 64, found[2], found[3]).astype(BF16)

    me = ep.astype(F32)

    def pack(k, first=0, last=4):
        with jax.named_scope(f"pack_{k}"):
            @pl.loop(first, last)
            def _(j):
                both = jnp.concatenate([MT[0, j, k], MT[1, j, k]], axis=1)
                shift = jnp.where(iota((1, 256), 1) >= 128, 64.0, 0.0)
                sl0 = jnp.where(both[0:1] == me, both[1:2] + shift, -1.0)
                sl1 = jnp.where(both[2:3] == me, both[3:4] + shift, -1.0)
                wt0 = both[4:5] + both[5:6] + both[6:7]
                wt1 = both[7:8] + both[8:9] + both[9:10]
                rows = iota((128, 256), 0).astype(F32)
                is0, is1 = rows == sl0, rows == sl1
                pick = jnp.where(is0 | is1, 1.0, 0.0)
                weight = jnp.sum(jnp.where(is0, wt0, 0.0) + jnp.where(is1, wt1, 0.0), axis=1, keepdims=True)
                r = pl.ds(pl.multiple_of(j * 128, 128), 128)
                WS[k, r, :] = jnp.broadcast_to(weight, (128, 128))
                PT[k, j] = jnp.transpose(pick).astype(BF16)
                pick = pick.astype(BF16)
                for n in range(4):
                    X[k, r, n * 512 : n * 512 + 512] = dot(
                        pick, T[k, j, :, n * 512 : n * 512 + 512]
                    ).astype(BF16)

    def packed(k):
        sent(f"y{k}")
        sent(f"d{k}")
        pl.semaphore_signal(ready.at[k], inc=1, device_id=sib, device_id_type=MESH)

    def pack_all(k):
        got_all(f"d{k}", T.at[k, :, 128:256])
        pack(k)
        packed(k)

    def gate_up(k, first, last, row=0, rows=512):
        with jax.named_scope(f"gate_up_{k}"):
            @pl.loop(first, last)
            def _(s):
                g = dot(X[k, row : row + rows], W[0, s])
                u = dot(X[k, row : row + rows], W[1, s])
                H[k, s, row : row + rows] = (g / (1.0 + jnp.exp(-g)) * u).astype(BF16)

    here[4].wait()
    with jax.named_scope("attend"):
        attend(0, 2)
    got_all("mz", MT.at[0, 0, 1:4])
    send("myr", MT.at[0, 0], MT.at[0, 3], yr, "my")
    send("myl", MT.at[0, 0], MT.at[0, 1], yl, "my")
    send("myo", MT.at[0, 0], MT.at[0, 2], yo, "my")
    with jax.named_scope("attend"):
        attend(2, 4)
    got("y0ra")
    send("y0fr", T.at[0, 3, 0:64], T.at[0, 2, 0:64], yr, "y0f")
    got("y0la")
    send("y0fl", T.at[0, 1, 64:128], T.at[0, 2, 64:128], yl, "y0f")
    with jax.named_scope("attend"):
        attend(4, 6)
    got("y0rb")
    send("d03", T.at[0, 3, 0:128], T.at[0, 3, 128:256], sib, "d0")
    got("y0lb")
    send("d01", T.at[0, 1, 0:128], T.at[0, 1, 128:256], sib, "d0")
    gather_start(1)
    gather_start(3)
    send_tile(2)
    got_all("halo", KV.at[:, :, 0 : 2 * WINDOW])
    with jax.named_scope("attend"):
        attend(6, 8)
    got_all("my", MT.at[0, 1:4])
    send("md", MT.at[0], MT.at[1], sib)
    with jax.named_scope("turn"):
        for kp in range(4):
            PMT[kp] = jnp.transpose(PM[kp].astype(F32)).astype(BF16)
    gather_end(0)
    got("md")
    pack_all(0)
    gate_up(0, 0, 1)
    pass_weight(0)
    gather_pass(1)
    gather_start(2)
    gather_pass(3)
    pass_weight(1)
    gather_end(1)
    gate_up(0, 1, 3)
    pack_all(1)
    gate_up(1, 0, 3)
    pass_down(0)
    start_down(1)
    start_down(2)
    gather_pass(2)
    got("d20", "d23", "d21")
    pack(2, 0, 2)
    pack(2, 3, 4)
    gate_up(2, 0, 3, 0, 256)
    gather_end(3)
    gate_up(2, 0, 3, 384, 128)
    pack_all(3)
    gate_up(3, 0, 1)
    gather_end(2)
    gate_up(3, 1, 3)
    got("d22")
    pack(2, 2, 3)
    packed(2)
    gate_up(2, 0, 3, 256, 128)
    for m in range(2):
        got_all(f"x{m}f", W.at[m, 3])
    gate_up(1, 3, 4)

    def down(c, k):
        with jax.named_scope(f"down_{c}{k}"):
            @pl.loop(0, CHUNKS[c][1] // 256)
            def _(n):
                cols = pl.ds(pl.multiple_of(CHUNKS[c][0] + n * 256, 256), 256)
                out = dot_nt(H[k, 0], W[2, 0, cols, :])
                for s in range(1, 4):
                    out += dot_nt(H[k, s], W[2, s, cols, :])
                scale = WS[k]
                scale = jnp.concatenate([scale, scale], axis=1)
                scaled = (out.astype(BF16).astype(F32) * scale).astype(BF16)
                for j in range(4):
                    part = dot(PT[k, j], scaled[j * 128 : j * 128 + 128])
                    X[k, j * 128 : j * 128 + 128, cols] = part[0:128].astype(BF16)
                    T[k, j, 128:256, cols] = part[128:256].astype(BF16)
        if c == 0:
            pl.semaphore_wait(ready.at[k], 1)
        cols = slice(CHUNKS[c][0], sum(CHUNKS[c]))
        send(f"r{c}{k}", T.at[k, :, 128:256, cols], T.at[k, :, 0:128, cols], sib)

    def plus(c, count, out, *terms):
        step = 16384 // CHUNKS[c][1]

        @pl.loop(0, count // step)
        def _(i):
            r = pl.multiple_of(i * step, step)

            def part(ref, lead, base):
                return (ref, (*lead, pl.ds(base + r, step), slice(CHUNKS[c][0], sum(CHUNKS[c]))))

            total = None
            for term in terms:
                ref, at = part(*term)
                value = ref[at].astype(F32)
                total = value if total is None else total + value
            ref, at = part(*out)
            ref[at] = total.astype(BF16)

    def early(c, k):
        cols = slice(CHUNKS[c][0], sum(CHUNKS[c]))
        got(f"r{c}{k}")
        for j in (2, 1, 3, 0):
            plus(c, 128, (X, (k,), j * 128), (X, (k,), j * 128), (T, (k, j), 0))
            if j == 2:
                send(f"b{c}{k}hr", X.at[k, 256:320, cols], R.at[k, 0, :, cols], yr, f"h{c}{k}", f"b{c}{k}")
                send(f"b{c}{k}hl", X.at[k, 320:384, cols], R.at[k, 1, :, cols], yl, f"h{c}{k}", f"b{c}{k}")
            if j == 1:
                send(f"b{c}{k}er", X.at[k, 192:256, cols], FB.at[k, 0, 64:128, cols], yr, f"F{c}{k}", f"b{c}{k}")
            if j == 3:
                send(f"b{c}{k}el", X.at[k, 384:448, cols], FB.at[k, 1, 0:64, cols], yl, f"F{c}{k}", f"b{c}{k}")

    def late(c, k):
        cols = slice(CHUNKS[c][0], sum(CHUNKS[c]))
        got_all(f"h{c}{k}", R.at[k, :, :, cols])
        plus(c, 64, (X, (k,), 128), (X, (k,), 128), (R, (k, 0), 0))
        send(f"b{c}{k}fr", X.at[k, 128:192, cols], FB.at[k, 0, 0:64, cols], yr, f"F{c}{k}", f"b{c}{k}")
        plus(c, 64, (X, (k,), 448), (X, (k,), 448), (R, (k, 1), 0))
        send(f"b{c}{k}fl", X.at[k, 448:512, cols], FB.at[k, 1, 64:128, cols], yl, f"F{c}{k}", f"b{c}{k}")

    def settle():
        unit, ref = done.pop(0)
        sent("r" + unit)
        sent_all("b" + unit, ref)

    def finish(c, k):
        cols = slice(CHUNKS[c][0], sum(CHUNKS[c]))
        got_all(f"F{c}{k}", FB.at[k, :, :, cols])
        out = (OUT, (0,), 0) if k == 0 else (S, (k - 1,), 0)
        plus(c, 128, out, (X, (k,), 0), (FB, (k, 0), 0), (FB, (k, 1), 0))
        if k:
            send(f"f{c}{k}", S.at[k - 1, :, cols], OUT.at[4 - k, :, cols], zs[k], f"f{c}")

        done.append((f"{c}{k}", X.at[k, 128:512, cols]))
        if len(done) > 1:
            settle()

    homes, done = [], []

    def restore(c):
        got_all(f"f{c}", OUT.at[1:4, :, slice(CHUNKS[c][0], sum(CHUNKS[c]))])
        first, width = CHUNKS[c]
        for piece in range(first // 256, (first + width) // 256):
            cols = slice(piece * 256, piece * 256 + 256)
            spot = (0, piece // 4)
            with jax.named_scope(f"restore_{c}"):
                for half in range(2):
                    total = None
                    for kp in range(4):
                        part = dot(PMT[kp, half * 256 : half * 256 + 256], OUT[kp, :, cols])
                        total = part if total is None else total + part
                    base = piece % 4 * 512 + half * 256
                    W[(*spot, slice(base, base + 256), slice(None))] = total.astype(BF16)
            base = piece % 4 * 512
            homes.append(local(20 + piece, W.at[0, piece // 4, base : base + 512], exp_out.at[:, cols]))

    half_rows = pl.ds(pl.multiple_of(core * 128, 128), 128)

    def start_out():
        here[6].wait()
        send("owr", OW.at[0, half_rows], OW.at[1, half_rows], xr)
        send("owl", OW.at[0, half_rows], OW.at[2, half_rows], xl)
        for name, d, slot, dev in (("ar", 1, 1, xr), ("al", 3, 2, xl), ("ao", 2, 3, xo)):
            part = pl.ds(pl.multiple_of(((tp + d) % 4) * 256, 256), 256)
            send(name, ATT.at[part], AR.at[slot], dev, "a")

    def pass_out():
        low = pl.ds(pl.multiple_of(core * 128, 64), 64)
        high = pl.ds(pl.multiple_of(core * 128 + 64, 64), 64)
        got("owr")
        send("owfr", OW.at[1, low], OW.at[3, low], xr, "owf")
        got("owl")
        send("owfl", OW.at[2, high], OW.at[3, high], xl, "owf")

    def share_out():
        got_all("owf", OW.at[3, half_rows])
        send("owd", OW.at[1:4, half_rows], OW.at[1:4, half_rows], sib)

    def project(half):
        if half == 0:
            got_all("a", AR.at[1:4])
            got("owd")
            here[7].wait()
            AR[0] = ATT[pl.ds(pl.multiple_of(tp * 256, 256), 256), :]
        with jax.named_scope("project"):
            r = slice(half * 128, half * 128 + 128)
            mixed = dot(AR[0, r, :], OW[0])
            for s in range(1, 4):
                mixed += dot(AR[s, r, :], OW[s])
            scale = lax.rsqrt(jnp.mean(mixed * mixed, axis=-1, keepdims=True) + EPS)
            mixed = (mixed * scale * OG[...]).astype(BF16)
            for piece in range(8):
                base = piece * 256 + half * 128
                W[1, 0, base : base + 128] = mixed[:, piece * 256 : piece * 256 + 256]
        if half == 1:
            for piece in range(8):
                base = piece * 256
                homes.append(local(12 + piece, W.at[1, 0, base : base + 256], mix_out.at[:, base : base + 256]))

    units = [(c, k) for c in range(2) for k in (1, 0, 3, 2)]
    units += [(2, 2), (2, 1), (2, 3), (2, 0)]
    units += [(3, 2), (3, 1), (3, 3), (4, 2), (4, 1), (4, 3), (3, 0), (4, 0)]
    arrived = set()

    def produce(i):
        c, k = units[i]
        if c not in arrived:
            arrived.add(c)
            first, width = CHUNKS[c]
            got_all(f"w{c}f", W.at[2, 3, first : first + width])
        down(c, k)

    produce(0)
    gate_up(0, 3, 4)
    produce(1)
    pass_down(1)
    early(*units[0])
    gate_up(3, 3, 4)
    early(*units[1])
    produce(2)
    early(*units[2])
    pass_down(2)
    start_down(3)
    start_down(4)
    gate_up(2, 3, 4)
    produce(3)
    late(*units[0])
    sent("z")

    hooks = {
        6: [lambda: sent("x"), lambda: sent("m")],
        9: [lambda: pass_down(3)],
        10: [lambda: pass_down(4), start_out],
        13: [lambda: restore(0)],
        15: [pass_out, lambda: sent("w"), lambda: restore(1)],
        17: [share_out],
        18: [lambda: restore(2)],
        19: [lambda: project(0)],
    }
    passed, ended = 1, 0
    for i in range(4, len(units)):
        produce(i)
        early(*units[i - 1])
        for hook in hooks.get(i, ()):
            hook()
        lag = 4 if i < 9 else 3 if i < 12 else 2
        while passed <= i - lag:
            late(*units[passed])
            passed += 1
        while ended <= i - lag - 3:
            finish(*units[ended])
            ended += 1
    early(*units[-1])
    project(1)
    finish(*units[-5])
    late(*units[-2])
    finish(*units[-4])
    late(*units[-1])
    finish(*units[-3])
    finish(*units[-2])
    restore(3)
    finish(*units[-1])
    restore(4)
    settle()
    sent("")
    assert len(numbers) == COPIES
    with jax.named_scope("home"):
        for copy in homes:
            copy.wait()


def local(
    queries, key_rows, values, sink_logit, out_weight, out_gain, routed_tokens,
    expert_ids, route_weight, routed_gain, expert_gate, expert_up, expert_down,
):
    anywhere = pl.BlockSpec(memory_space=pl.ANY)
    vmem = pl.BlockSpec(memory_space=pltpu.VMEM)
    smem = pl.BlockSpec(memory_space=pltpu.SMEM)
    scratch = [
        pltpu.VMEM((3, 4, 2048, 256), BF16),
        pltpu.VMEM((4, 256, D), BF16),
        pltpu.VMEM((4, 4, 256, D), BF16),
        pltpu.VMEM((4, 512, D), BF16),
        pltpu.VMEM((4, 4, 512, 256), BF16),
        pltpu.VMEM((4, 2, 64, D), BF16),
        pltpu.VMEM((4, 2, 128, D), BF16),
        pltpu.VMEM((3, 128, D), BF16),
        pltpu.VMEM((4, 128, D), BF16),
        pltpu.VMEM((4, 512, 128), F32),
        pltpu.VMEM((4, 4, 256, 128), BF16),
        pltpu.VMEM((4, 128, 512), BF16),
        pltpu.VMEM((4, 512, 128), BF16),
        pltpu.VMEM((2, 4, 4, 16, 128), F32),
        pltpu.VMEM((3, 16, 128), F32),
        pltpu.VMEM((1024, 256), BF16),
        pltpu.VMEM((2, 128, 1024 + 2 * WINDOW), BF16),
        pltpu.VMEM((1024, 256), BF16),
        pltpu.VMEM((4, 256, 256), BF16),
        pltpu.VMEM((1, D), F32),
        pltpu.VMEM((1, D), F32),
        pltpu.SemaphoreType.REGULAR((4,)),
        pltpu.SemaphoreType.DMA((28,)),
        pltpu.SemaphoreType.DMA((SENDS,)),
        pltpu.SemaphoreType.DMA((COPIES,)),
    ]
    return pl.pallas_call(
        kernel,
        out_shape=(
            jax.ShapeDtypeStruct((256, D), BF16),
            jax.ShapeDtypeStruct((512, D), BF16),
        ),
        in_specs=[
            anywhere, anywhere, anywhere, smem, anywhere, anywhere, anywhere, vmem, vmem,
            anywhere, anywhere, anywhere, anywhere,
        ],
        out_specs=(anywhere, anywhere),
        scratch_shapes=scratch,
        compiler_params=pltpu.CompilerParams(
            collective_id=0, has_side_effects=True, vmem_limit_bytes=67043328
        ),
        name="block",
    )(
        queries, key_rows.T, values.T, sink_logit, out_weight, out_gain.reshape(1, D), routed_tokens,
        expert_ids.T, route_weight.T, routed_gain.reshape(1, D), expert_gate.reshape(D, 256),
        expert_up.reshape(D, 256), expert_down.reshape(D, 256),
    )


def solution(mesh):
    placed = (
        P("ep", "tp"), P("ep", "tp"), P("ep", "tp"), P("tp"), P("tp", None), P(),
        P(("ep", "tp"), None), P(("ep", "tp"), None), P(("ep", "tp"), None), P(),
        P("ep", None, "tp"), P("ep", None, "tp"), P("ep", None, "tp"),
    )
    return jax.shard_map(
        local,
        mesh=mesh,
        in_specs=placed,
        out_specs=(P(("ep", "tp"), None), P(("ep", "tp"), None)),
        check_vma=False,
    )
```
